768 devices in a mesh: sp: 192 (over z, y, core), tp: 4 (over x).
Axes of the slice: x: 4, y: 8, z: 12, core: 2. Of those that a mesh axis runs over, the one named last changes fastest.
Arguments:
- tokens: bfloat16 [1, 98304, 2048], P(None, ('sp', 'tp')), may hold values from -6 to 6
- input_norm_gain: float32 [2048], replicated, may hold values from 0.1 to 1.9
- query_weight: bfloat16 [2048, 1024], P(None, 'tp'), may hold values from -0.125 to 0.125
- forget_weight: bfloat16 [2048, 1024], P(None, 'tp'), may hold values from -0.125 to 0.125
- input_weight: bfloat16 [2048, 1024], P(None, 'tp'), may hold values from -0.125 to 0.125
- gate_weight: bfloat16 [2048, 1024], P(None, 'tp'), may hold values from -0.125 to 0.125
- slack: float32 [1024], P('tp'), may hold values from 0 to 0.06
- sudden_decay: float32 [1, 98304, 8], P(None, 'sp', 'tp'), may hold values from -0.75 to 0
- head_norm_gain: float32 [128], replicated, may hold values from 0.1 to 1.9
- output_weight: bfloat16 [1024, 2048], P(None, 'tp'), may hold values from -1.25 to 1.25
- output_norm_gain: float32 [2048], P('tp'), may hold values from 0.1 to 1.9
Outputs:
- mixer_output: bfloat16 [1, 98304, 2048], P(None, 'sp', 'tp')
The draws below stay inside these ranges and needn't reach their ends.
All inputs are finite; a program needn't handle non-finite values.
Results may differ from the reference program's by a relative error of at most 0.0094.
Values may be sent and summed in bfloat16 or wider, within the bound.
A program may use at most 64 MiB of HBM per device.

```python
import math
import jax
import jax.numpy as jnp
from jax import lax

D = 2048
HEADS = 8
KEY = 128
VAL = 128
BLOCK = 64
SEQUENCE_COUNT = 1
TOKENS_PER_SHARD = 512
SEQUENCE_LENGTH = 98304


def head_plan(key):
    head_order = jax.random.permutation(jax.random.fold_in(key, 101), HEADS)
    fast_count = HEADS // 2
    return head_order < fast_count


def spread_draw(key, lowest, highest, extent):
    return jnp.exp(jax.random.uniform(key, extent, jnp.float32, math.log(lowest), math.log(highest)))


def draw_slack(key, part):
    fast_heads = head_plan(key)
    quick_rate = spread_draw(jax.random.fold_in(key, 1), 0.02, 0.06, (HEADS, KEY))
    slow_rate = spread_draw(jax.random.fold_in(key, 2), 0.2 / SEQUENCE_LENGTH, 0.6 / SEQUENCE_LENGTH, (HEADS, KEY))
    return jnp.where(fast_heads[:, None], quick_rate, slow_rate).reshape(HEADS * KEY).astype(jnp.float32)


def draw_sudden_decay(key, part):
    fast_heads = head_plan(key)
    per_head_rate = jnp.where(fast_heads, spread_draw(jax.random.fold_in(key, 3), 0.005, 0.02, (HEADS,)), spread_draw(jax.random.fold_in(key, 4), 0.2 / SEQUENCE_LENGTH, 0.5 / SEQUENCE_LENGTH, (HEADS,)))
    multiplier = spread_draw(jax.random.fold_in(key, 5), 0.25, 2.0, (SEQUENCE_COUNT, SEQUENCE_LENGTH // TOKENS_PER_SHARD))
    multiplier = jnp.repeat(multiplier, TOKENS_PER_SHARD, axis=1)
    sudden_positions = jax.random.randint(jax.random.fold_in(key, 6), (SEQUENCE_COUNT, 2), 0, SEQUENCE_LENGTH)
    sudden_loss = jax.random.uniform(jax.random.fold_in(key, 7), (SEQUENCE_COUNT, 2), jnp.float32, 0.2, 0.5)
    locations = jnp.arange(SEQUENCE_LENGTH)[None, :, None]
    sudden_drops = jnp.sum(jnp.where(locations == sudden_positions[:, None, :], jnp.log(1.0 - sudden_loss)[:, None, :], 0.0), axis=2)
    return (sudden_drops[:, :, None] - per_head_rate[None, None, :] * multiplier[:, :, None]).astype(jnp.float32)


def draw_output_weight(key, part):
    columns = jnp.arange(D, dtype=jnp.float32) / D
    jitter = jax.random.uniform(jax.random.fold_in(key, 8), (D,), jnp.float32)
    exponent = 0.5 * columns + 0.5 * jitter
    entries = jax.random.truncated_normal(jax.random.fold_in(key, 9), -4.0, 4.0, (HEADS * VAL, D), jnp.float32)
    return (entries * (10.0 ** exponent)[None, :] * (HEADS * VAL) ** (-0.5)).astype(jnp.bfloat16)


def shard_levels(own_key, shape, cuts, least, largest):
    factor_of = 1.0
    for axis_at, parts in cuts:
        steps = jax.random.uniform(jax.random.fold_in(jax.random.fold_in(own_key, 6), axis_at), (parts,), jnp.float32, least / len(cuts), largest / len(cuts))
        factor_of = factor_of * jnp.repeat(jnp.exp(steps), shape[axis_at] // parts).reshape((-1,) + (1,) * (len(shape) - 1 - axis_at))
    return factor_of


def gaussian(stream_key, dims, spread, most, cuts=(), held_as=jnp.bfloat16):
    array = spread * jax.random.normal(stream_key, dims, jnp.float32)
    if cuts:
        array = array * shard_levels(stream_key, dims, cuts, -0.22, 0.18)
    return jnp.clip(array, -most, most).astype(held_as)


def setup_inputs(seed: int = 0) -> dict:
    splits = jax.random.split(jax.random.key(seed), 12)
    return {
        "tokens": gaussian(splits[0], (SEQUENCE_COUNT, SEQUENCE_LENGTH, D), 1.0, 6.0, ((1, 768),)),
        "input_norm_gain": jnp.clip(1.0 + 0.18 * jax.random.normal(splits[1], (D,), jnp.float32), 0.1, 1.9),
        "query_weight": gaussian(splits[2], (D, HEADS * KEY), D ** -0.5, 0.125, ((1, 4),)),
        "forget_weight": gaussian(splits[3], (D, HEADS * KEY), D ** -0.5, 0.125, ((1, 4),)),
        "input_weight": gaussian(splits[4], (D, HEADS * VAL), D ** -0.5, 0.125, ((1, 4),)),
        "gate_weight": gaussian(splits[5], (D, HEADS * VAL), D ** -0.5, 0.125, ((1, 4),)),
        "slack": draw_slack(jax.random.fold_in(splits[11], 71), 0),
        "sudden_decay": draw_sudden_decay(jax.random.fold_in(splits[11], 71), 0),
        "head_norm_gain": jnp.clip(1.0 + 0.18 * jax.random.normal(splits[8], (VAL,), jnp.float32), 0.1, 1.9),
        "output_weight": draw_output_weight(jax.random.fold_in(splits[11], 71), 0),
        "output_norm_gain": jnp.clip(1.0 + 0.18 * jax.random.normal(splits[10], (D,), jnp.float32), 0.1, 1.9),
    }


epsilon = 1e-06
precise = lax.Precision.HIGHEST

def normalize(tensor_in, gain_vec):
    tensor_in = tensor_in.astype(jnp.float32)
    return tensor_in * lax.rsqrt(lax.optimization_barrier(jnp.mean(tensor_in * tensor_in, axis=-1, keepdims=True)) + epsilon) * gain_vec

def setup_params(query_logits, forget_logits, input_logits, slack, sudden_decay):
    sequence_total, sequence_span, local_heads = sudden_decay.shape

    def heads_first(tensor):
        return tensor.astype(jnp.float32).reshape(sequence_total, sequence_span, local_heads, -1).transpose(0, 2, 1, 3)
    query_rows = heads_first(query_logits) * KEY ** (-0.5)
    incoming_weights = slack.reshape(local_heads, -1)[None, :, None, :] * jax.nn.sigmoid(-heads_first(forget_logits))
    forget_logarithm = jnp.log1p(-incoming_weights) + sudden_decay.transpose(0, 2, 1)[:, :, :, None]
    return (query_rows, incoming_weights, heads_first(input_logits), forget_logarithm)

def block_pass(query_rows, incoming_weights, value_rows, forget_logarithm, initial):
    sequence_total, local_heads, sequence_span, key_width = query_rows.shape
    blocks_here = sequence_span // BLOCK

    def by_block(tensor):
        return tensor.reshape(sequence_total, local_heads, blocks_here, BLOCK, tensor.shape[3]).transpose(2, 0, 1, 3, 4)
    causal = jnp.tril(jnp.ones((BLOCK, BLOCK), dtype=bool))

    def advance(carried, portions):
        query_blk, weight_blk, value_blk, forget_blk = portions
        running = jnp.cumsum(forget_blk, axis=2)
        lifted_q = query_blk * jnp.exp(running)
        lifted_k = weight_blk * jnp.exp(-running)
        scores = jnp.einsum('shtk,shuk->shtu', lifted_q, lifted_k, precision=precise)
        scores = jnp.where(causal, scores, 0.0)
        produced = jnp.einsum('shtu,shuv->shtv', scores, value_blk, precision=precise) + jnp.einsum('shtk,shkv->shtv', lifted_q, carried, precision=precise)
        ending = running[:, :, -1:, :]
        carried = jnp.exp(ending[:, :, 0, :])[..., None] * carried + jnp.einsum('shuk,shuv->shkv', weight_blk * jnp.exp(ending - running), value_blk, precision=precise)
        return (carried, produced)
    final_state, produced = lax.scan(advance, initial, (by_block(query_rows), by_block(incoming_weights), by_block(value_rows), by_block(forget_logarithm)))
    return (final_state, produced.transpose(1, 2, 0, 3, 4).reshape(sequence_total, local_heads, sequence_span, value_rows.shape[3]))

def gate_heads(produced, gate_raw, head_norm_gain):
    sequence_total, local_heads, sequence_span, val_width = produced.shape
    mean_sq = lax.optimization_barrier(jnp.mean(produced * produced, axis=3, keepdims=True))
    scaled = produced * lax.rsqrt(mean_sq + epsilon) * head_norm_gain
    scaled = scaled.transpose(0, 2, 1, 3).reshape(sequence_total, sequence_span, local_heads * val_width)
    return (scaled * jax.nn.silu(gate_raw.astype(jnp.float32))).astype(jnp.bfloat16)

def reference(tokens, input_norm_gain, query_weight, forget_weight, input_weight, gate_weight, slack, sudden_decay, head_norm_gain, output_weight, output_norm_gain):
    sequence_total, sequence_span, model_width = tokens.shape
    matrices = [matrix.astype(jnp.float32) for matrix in (query_weight, forget_weight, input_weight, gate_weight)]
    out_matrix = output_weight.astype(jnp.float32)
    segments = sequence_span // TOKENS_PER_SHARD

    def segment(carried, seg_index):
        leading_row = (seg_index * TOKENS_PER_SHARD).astype(jnp.int32)
        token_rows = lax.dynamic_slice_in_dim(tokens, leading_row, TOKENS_PER_SHARD, 1)
        normed = normalize(token_rows, input_norm_gain).astype(jnp.bfloat16)
        normed = lax.optimization_barrier(normed).astype(jnp.float32)
        unprocessed_parts = [lax.optimization_barrier(jnp.einsum('std,dc->stc', normed, matrix).astype(jnp.bfloat16)) for matrix in matrices]
        sudden_rows = lax.dynamic_slice_in_dim(sudden_decay, leading_row, TOKENS_PER_SHARD, 1)
        query_rows, incoming_weights, value_rows, forget_logarithm = setup_params(unprocessed_parts[0], unprocessed_parts[1], unprocessed_parts[2], slack, sudden_rows)
        carried, produced = block_pass(query_rows, incoming_weights, value_rows, forget_logarithm, carried)
        gated_out = lax.optimization_barrier(gate_heads(produced, unprocessed_parts[3], head_norm_gain)).astype(jnp.float32)
        projected = jnp.einsum('stc,cd->std', gated_out, out_matrix)
        return (carried, normalize(projected, output_norm_gain).astype(jnp.bfloat16))
    initial = jnp.zeros((sequence_total, HEADS, KEY, VAL), jnp.float32)
    _, outputs = lax.scan(segment, initial, jnp.arange(segments, dtype=jnp.int32))
    return outputs.transpose(1, 0, 2, 3).reshape(sequence_total, sequence_span, model_width)
```

```python
import jax
import jax.numpy as jnp
from jax import lax
from jax.experimental import pallas as pl
from jax.experimental.pallas import tpu as pltpu
from jax.sharding import Mesh
from jax.sharding import PartitionSpec as P

D = 2048
KEY = 128
SP = ("sp_0", "sp_1", "sp_2")
SP_TP = ("sp_0", "sp_1", "sp_2", "tp")
MESH = pl.DeviceIdType.MESH
EPS = 1e-06

NZ, NY, NC, NX = 12, 8, 2, 4
NM = NY * NC
T = 128
H = T // 2
NB = 4
W2 = 256
PIECE = 256 // NM
MSG = PIECE + 8

bf16 = jnp.bfloat16
f32 = jnp.float32


def dot(a, b, ca=1, cb=0):
    return lax.dot_general(a, b, (((ca,), (cb,)), ((), ())), preferred_element_type=f32)


def split3(x):
    hi = x.astype(bf16).astype(f32)
    rest = x - hi
    mid = rest.astype(bf16).astype(f32)
    return hi, mid, rest - mid


def decay_rows(row):
    hi, mid, lo = split3(row)
    at = lax.broadcasted_iota(jnp.int32, (8, 128), 0)
    rows = jnp.where(at == 0, hi, jnp.where(at == 1, mid, jnp.where(at == 2, lo, 0.0)))
    return rows.astype(bf16)


def body(
    tokens, ing, wq, wf, wi, wg, slack, sud, hgain, wo, ogain, out,
    xin, G, W, WO, lqA, lk, vv, lqD, gs, ST, PB, DT, DP, BC, O,
    msgA, rA, Pp, zout, rz, rout, SIN, GG, PJ, sqo, sqr,
    ldsem, gsR, grR, gsL, grL, sA, qA, sZ, qZ, sR, qR, hsR, hrR, hsL, hrL, sS, qS,
):
    X = lax.axis_index("tp")
    Z = lax.axis_index("sp_0")
    Y = lax.axis_index("sp_1")
    C = lax.axis_index("sp_2")
    M = Y * NC + C
    right = lax.rem(X + 1, NX)
    left = lax.rem(X + NX - 1, NX)
    opp = lax.rem(X + 2, NX)

    def member(m):
        return {"sp_1": m // NC, "sp_2": lax.rem(m, NC)}

    ld_tok = pltpu.make_async_copy(tokens.at[0], xin, ldsem.at[0])
    ld_tok.start()
    loads = [pltpu.make_async_copy(w, W.at[i], ldsem.at[1 + i]) for i, w in enumerate((wq, wf, wi, wg))]
    ld_wo = pltpu.make_async_copy(wo, WO, ldsem.at[5])
    for c in loads:
        c.start()
    ld_wo.start()

    barrier = pltpu.get_barrier_semaphore()
    for dx in range(1, NX):
        pl.semaphore_signal(barrier, inc=1, device_id={"tp": lax.rem(X + dx, NX)}, device_id_type=MESH)
    for dm in range(1, NM):
        pl.semaphore_signal(barrier, inc=1, device_id=member(lax.rem(M + dm, NM)), device_id_type=MESH)
    for dz in range(1, NZ):
        pl.semaphore_signal(barrier, inc=1, device_id={"sp_0": lax.rem(Z + dz, NZ)}, device_id_type=MESH)

    ld_tok.wait()

    def norm_rows(i, _):
        rows = xin[pl.ds(pl.multiple_of(i * 16, 16), 16), :].astype(f32)
        rows = rows * lax.rsqrt(jnp.mean(rows * rows, axis=1, keepdims=True) + EPS) * ing[...]
        G[X, i // 4, pl.ds(pl.multiple_of(lax.rem(i, 4) * 16, 16), 16), :] = rows.astype(bf16)
        return 0

    lax.fori_loop(0, T // 16, norm_rows, 0)
    pl.semaphore_wait(barrier, (NX - 1) + (NM - 1) + (NZ - 1))

    def to_right(who, half, slot):
        return pltpu.make_async_remote_copy(
            G.at[who, half], G.at[who, half], gsR.at[slot], grR.at[slot], device_id={"tp": right}, device_id_type=MESH
        )

    def to_left(who, half, slot):
        return pltpu.make_async_remote_copy(
            G.at[who, half], G.at[who, half], gsL.at[slot], grL.at[slot], device_id={"tp": left}, device_id_type=MESH
        )

    to_right(X, 0, 0).start()
    to_left(X, 1, 0).start()
    to_right(X, 1, 1).start()
    to_left(X, 0, 1).start()

    t_at = lax.broadcasted_iota(jnp.int32, (T, T), 0)
    s_at = lax.broadcasted_iota(jnp.int32, (T, T), 1)
    causal = s_at <= t_at
    tri = causal.astype(f32).astype(bf16)
    for b in range(NB):
        for h in range(2):
            line = jnp.broadcast_to(sud[h : h + 1, b * T : (b + 1) * T], (T, T))
            total = jnp.sum(jnp.where(causal, line, 0.0), axis=1, keepdims=True)
            BC[b, h] = jnp.broadcast_to(total, (T, T))

    for c in loads:
        c.wait()

    def block(b):
        x = G[b].reshape(T, D)
        f_raw = dot(x, W[1]).astype(bf16).astype(f32)
        i_raw = dot(x, W[2]).astype(bf16)
        vv[b] = i_raw
        w = slack[...] * jax.nn.sigmoid(-f_raw)
        a = jnp.log1p(-w)
        a_hi = a.astype(bf16)
        a_lo = (a - a_hi.astype(f32)).astype(bf16)
        A = dot(tri, a_hi) + dot(tri, a_lo)
        lk[b] = (w * jnp.exp(-A)).astype(bf16)
        for h in range(2):
            cols = slice(h * 128, (h + 1) * 128)
            reach = A[:, cols] + BC[b, h]
            end = reach[T - 1 : T, :]
            DT[b, h : h + 1, :] = end
            wk = (w[:, cols] * jnp.exp(end - reach)).astype(bf16)
            ST[b, h] = dot(i_raw[:, cols], wk, 0, 0)
        q_raw = dot(x, W[0]).astype(bf16).astype(f32) * KEY ** (-0.5)
        q_in = q_raw * jnp.exp(A)
        lqA[b] = q_in.astype(bf16)
        for h in range(2):
            cols = slice(h * 128, (h + 1) * 128)
            lqD[b, :, cols] = q_in[:, cols] * jnp.exp(BC[b, h])
        g_raw = dot(x, W[3]).astype(bf16).astype(f32)
        silu = g_raw * jax.nn.sigmoid(g_raw)
        for h in range(2):
            cols = slice(h * 128, (h + 1) * 128)
            gs[b, :, cols] = silu[:, cols] * hgain[...]

    def arrive(i, _):
        @pl.when(i == 1)
        def _():
            to_right(X, 0, 0).wait_recv()
            to_right(left, 0, 2).start()
            to_left(X, 1, 0).wait_recv()
            to_left(right, 1, 2).start()
            to_right(X, 1, 1).wait_recv()
            to_left(X, 0, 1).wait_recv()

        @pl.when(i == 3)
        def _():
            to_right(left, 0, 2).wait_recv()
            to_left(right, 1, 2).wait_recv()

        block(lax.rem(X + 3 * i + 3 * (i // 2) + 2 * (i // 3), NX))
        return 0

    lax.fori_loop(0, NB, arrive, 0)

    finals, totals = [], []
    for h in range(2):
        state = jnp.zeros((128, 128), f32)
        reach = jnp.zeros((1, 128), f32)
        for b in range(NB):
            PB[b, h] = state.astype(bf16)
            DP[b, h : h + 1, :] = reach
            step = DT[b, h : h + 1, :]
            state = jnp.exp(step) * state + ST[b, h]
            reach = reach + step
        finals.append(state)
        totals.append(reach)
    for h in range(2):
        rows = decay_rows(totals[h])
        for j in range(NM // 2):
            m = h * (NM // 2) + j
            msgA[m, 0:PIECE, :] = finals[h][j * PIECE : (j + 1) * PIECE, :].astype(bf16)
            msgA[m, PIECE:MSG, :] = rows

    far_first = sorted(range(1, NM), key=lambda d: -min(d // 2, NY - d // 2))

    def piece_to(dm):
        m = lax.rem(M + dm, NM)
        return pltpu.make_async_remote_copy(
            msgA.at[m], rA.at[M], sA.at[dm], qA.at[dm], device_id=member(m), device_id_type=MESH
        )

    for dm in far_first:
        piece_to(dm).start()
    rA[M] = msgA[M]

    def inner(b, _):
        for h in range(2):
            cols = slice(h * 128, (h + 1) * 128)
            bc = BC[b, h]
            scores = dot(lqA[b, :, cols], lk[b, :, cols], 1, 1)
            scores = scores * jnp.exp(jnp.where(causal, bc - bc.T, -1e30))
            scores = jnp.where(causal, scores, 0.0)
            q_in = lqD[b, :, cols]
            O[b, :, cols] = dot(scores.astype(bf16), vv[b, :, cols]) + dot(q_in.astype(bf16), PB[b, h], 1, 1)
            lqA[b, :, cols] = (q_in * jnp.exp(DP[b, h : h + 1, :])).astype(bf16)
        return 0

    lax.fori_loop(0, NB, inner, 0)

    for dm in range(1, NM):
        piece_to(dm).wait_recv()

    def decay_of(rows):
        part = rows[PIECE:MSG, :].astype(f32)
        return part[0:1, :] + part[1:2, :] + part[2:3, :]

    state = jnp.zeros((PIECE, 128), f32)
    reach = jnp.zeros((1, 128), f32)
    reaches = []
    for m in range(NM):
        rows = rA[m]
        Pp[m] = state
        reaches.append(reach)
        step = decay_of(rows)
        state = jnp.exp(step) * state + rows[0:PIECE, :].astype(f32)
        reach = reach + step
    zout[0:PIECE, :] = state.astype(bf16)
    zout[PIECE:MSG, :] = decay_rows(reach)

    def row_to(z):
        return pltpu.make_async_remote_copy(
            zout, rz.at[Z], sZ.at[z], qZ.at[Z], device_id={"sp_0": z}, device_id_type=MESH
        )

    def row_from(z):
        return pltpu.make_async_remote_copy(
            zout, rz.at[z], sZ.at[z], qZ.at[z], device_id={"sp_0": z}, device_id_type=MESH
        )

    def send_row(z, _):
        row_to(z).start()
        return 0

    lax.fori_loop(Z + 1, NZ, send_row, 0)

    def take_row(z, before):
        row_from(z).wait_recv()
        rows = rz[z]
        return jnp.exp(decay_of(rows)) * before + rows[0:PIECE, :].astype(f32)

    before = lax.fori_loop(0, Z, take_row, jnp.zeros((PIECE, 128), f32))
    for m in range(NM):
        rout[m] = (jnp.exp(reaches[m]) * before + Pp[m]).astype(bf16)

    def back_to(dm):
        m = lax.rem(M + dm, NM)
        return pltpu.make_async_remote_copy(
            rout.at[m], SIN.at[M], sR.at[dm], qR.at[dm], device_id=member(m), device_id_type=MESH
        )

    for dm in far_first:
        back_to(dm).start()
    SIN[M] = rout[M]
    for dm in range(1, NM):
        back_to(dm).wait_recv()

    def h_right(who, r, half, slot):
        return pltpu.make_async_remote_copy(
            GG.at[who, r, half], GG.at[who, r, half], hsR.at[r, slot], hrR.at[r, slot],
            device_id={"tp": right}, device_id_type=MESH,
        )

    def h_left(who, r, half, slot):
        return pltpu.make_async_remote_copy(
            GG.at[who, r, half], GG.at[who, r, half], hsL.at[r, slot], hrL.at[r, slot],
            device_id={"tp": left}, device_id_type=MESH,
        )

    def readout(r, _):
        parts = []
        for h in range(2):
            cols = slice(h * 128, (h + 1) * 128)
            carried = SIN[h * 8 : (h + 1) * 8].reshape(128, 128)
            o = O[r, :, cols] + dot(lqA[r, :, cols], carried, 1, 1)
            o = o * lax.rsqrt(jnp.mean(o * o, axis=1, keepdims=True) + EPS)
            parts.append(o * gs[r, :, cols])
        gated = jnp.concatenate(parts, axis=1).astype(bf16)
        GG[X, r] = gated.reshape(2, H, W2)
        h_right(X, r, 0, 0).start()
        h_left(X, r, 1, 0).start()
        h_right(X, r, 1, 1).start()
        h_left(X, r, 0, 1).start()
        return 0

    lax.fori_loop(0, NB, readout, 0)
    ld_wo.wait()

    def forward(r):
        h_right(X, r, 0, 0).wait_recv()
        h_right(left, r, 0, 2).start()
        h_left(X, r, 1, 0).wait_recv()
        h_left(right, r, 1, 2).start()

    def square_to(dx, r):
        return pltpu.make_async_remote_copy(
            sqo.at[r], sqr.at[dx - 1, r], sS.at[dx - 1, r], qS.at[dx - 1, r],
            device_id={"tp": lax.rem(X + dx, NX)}, device_id_type=MESH,
        )

    def project(r, _):
        @pl.when(r < NB - 1)
        def _():
            forward(r + 1)

        h_right(X, r, 1, 1).wait_recv()
        h_left(X, r, 0, 1).wait_recv()
        h_right(left, r, 0, 2).wait_recv()
        h_left(right, r, 1, 2).wait_recv()
        acc = dot(GG[0, r].reshape(T, W2), WO[0:W2, :])
        for j in range(1, NX):
            acc = acc + dot(GG[j, r].reshape(T, W2), WO[j * W2 : (j + 1) * W2, :])
        PJ[r] = acc
        sq = acc * acc
        sq_hi = sq.astype(bf16)
        sq_lo = (sq - sq_hi.astype(f32)).astype(bf16)
        ones = jnp.ones((8, 512), f32).astype(bf16)
        sqo[r] = dot(ones, sq_hi, 1, 1) + dot(ones, sq_lo, 1, 1)
        for dx in (2, 1, 3):
            square_to(dx, r).start()
        return 0

    forward(0)
    lax.fori_loop(0, NB, project, 0)

    def finish(r, _):
        for dx in (1, 2, 3):
            square_to(dx, r).wait_recv()
        total = sqo[r] + sqr[0, r] + sqr[1, r] + sqr[2, r]
        scale = lax.rsqrt(total[0:1, :] / D + EPS)
        scale = jnp.broadcast_to(scale, (T, T)).T
        for j in range(4):
            cols = slice(j * 128, (j + 1) * 128)
            out[0, pl.ds(pl.multiple_of(r * T, T), T), cols] = (
                PJ[r, :, cols] * scale * ogain[:, cols]
            ).astype(bf16)
        return 0

    lax.fori_loop(0, NB, finish, 0)

    to_right(X, 0, 0).wait_send()
    to_right(X, 1, 1).wait_send()
    to_right(left, 0, 2).wait_send()
    to_left(X, 1, 0).wait_send()
    to_left(X, 0, 1).wait_send()
    to_left(right, 1, 2).wait_send()
    for dm in range(1, NM):
        piece_to(dm).wait_send()
        back_to(dm).wait_send()

    def row_left(z, _):
        row_to(z).wait_send()
        return 0

    lax.fori_loop(Z + 1, NZ, row_left, 0)

    def rest(r, _):
        h_right(X, r, 0, 0).wait_send()
        h_right(X, r, 1, 1).wait_send()
        h_right(left, r, 0, 2).wait_send()
        h_left(X, r, 1, 0).wait_send()
        h_left(X, r, 0, 1).wait_send()
        h_left(right, r, 1, 2).wait_send()
        for dx in (1, 2, 3):
            square_to(dx, r).wait_send()
        return 0

    lax.fori_loop(0, NB, rest, 0)


def shards(tokens, ing, wq, wf, wi, wg, slack, sud, hgain, wo, ogain):
    vm = pl.BlockSpec(memory_space=pltpu.VMEM)
    hb = pl.BlockSpec(memory_space=pl.ANY)
    dma = pltpu.SemaphoreType.DMA
    V = pltpu.VMEM
    return pl.pallas_call(
        body,
        name="layer",
        out_shape=jax.ShapeDtypeStruct((1, 512, 512), bf16),
        in_specs=[hb, vm, hb, hb, hb, hb, vm, vm, vm, hb, vm],
        out_specs=vm,
        scratch_shapes=[
            V((T, D), bf16),
            V((NX, 2, H, D), bf16),
            V((4, D, W2), bf16),
            V((1024, 512), bf16),
            V((NB, T, W2), bf16),
            V((NB, T, W2), bf16),
            V((NB, T, W2), bf16),
            V((NB, T, W2), f32),
            V((NB, T, W2), f32),
            V((NB, 2, 128, 128), f32),
            V((NB, 2, 128, 128), bf16),
            V((NB, 2, 128), f32),
            V((NB, 2, 128), f32),
            V((NB, 2, T, T), f32),
            V((NB, T, W2), f32),
            V((NM, MSG, 128), bf16),
            V((NM, MSG, 128), bf16),
            V((NM, PIECE, 128), f32),
            V((MSG, 128), bf16),
            V((NZ, MSG, 128), bf16),
            V((NM, PIECE, 128), bf16),
            V((NM, PIECE, 128), bf16),
            V((NX, NB, 2, H, W2), bf16),
            V((NB, T, 512), f32),
            V((NB, 8, 128), f32),
            V((3, NB, 8, 128), f32),
            dma((6,)),
            dma((3,)), dma((3,)), dma((3,)), dma((3,)),
            dma((NM,)), dma((NM,)),
            dma((NZ,)), dma((NZ,)),
            dma((NM,)), dma((NM,)),
            dma((NB, 3)), dma((NB, 3)), dma((NB, 3)), dma((NB, 3)),
            dma((3, NB)), dma((3, NB)),
        ],
        compiler_params=pltpu.CompilerParams(
            collective_id=0, has_side_effects=True, vmem_limit_bytes=60 * 1024 * 1024
        ),
    )(
        tokens,
        ing.reshape(1, D),
        wq, wf, wi, wg,
        slack.reshape(1, W2),
        sud[0].T,
        hgain.reshape(1, 128),
        wo,
        ogain.reshape(1, 512),
    )


def solution(mesh):
    torus = Mesh(mesh.devices.reshape(NZ, NY, NC, NX), ("sp_0", "sp_1", "sp_2", "tp"))
    in_specs = (
        P(None, SP_TP, None),
        P(),
        P(None, "tp"),
        P(None, "tp"),
        P(None, "tp"),
        P(None, "tp"),
        P("tp"),
        P(None, SP, "tp"),
        P(),
        P(None, "tp"),
        P("tp"),
    )
    out_specs = P(None, SP, "tp")
    return jax.shard_map(shards, mesh=torus, in_specs=in_specs, out_specs=out_specs, check_vma=False)
```

```python
import jax
import jax.numpy as jnp
from jax import lax
from jax.experimental import pallas as pl
from jax.experimental.pallas import tpu as pltpu
from jax.sharding import Mesh
from jax.sharding import PartitionSpec as P

D = 2048
KEY = 128
SP = ("sp_0", "sp_1", "sp_2")
SP_TP = ("sp_0", "sp_1", "sp_2", "tp")
MESH = pl.DeviceIdType.MESH
EPS = 1e-06

NZ, NY, NC, NX = 12, 8, 2, 4
NM = NY * NC
T = 128
H = T // 2
Q = T // 4
OUTER = (0, 3, 1, 2)
NB = 4
W2 = 256
PIECE = 256 // NM
MSG = PIECE + 8

bf16 = jnp.bfloat16
f32 = jnp.float32


def dot(a, b, ca=1, cb=0):
    return lax.dot_general(a, b, (((ca,), (cb,)), ((), ())), preferred_element_type=f32)


def split3(x):
    hi = x.astype(bf16).astype(f32)
    rest = x - hi
    mid = rest.astype(bf16).astype(f32)
    return hi, mid, rest - mid


def decay_rows(row):
    hi, mid, lo = split3(row)
    at = lax.broadcasted_iota(jnp.int32, (8, 128), 0)
    rows = jnp.where(at == 0, hi, jnp.where(at == 1, mid, jnp.where(at == 2, lo, 0.0)))
    return rows.astype(bf16)


def body(
    tokens, ing_in, wq, wf, wi, wg, slack_in, sud_in, hgain_in, wo, ogain_in, out,
    ing, slack, sud, hgain, ogain,
    xin, G, W, WO, lqA, lk, vv, lqD, gs, ST, PB, DT, DP, BC, AA, O,
    msgA, rA, Pp, zout, rz, rout, SIN, GG, PJ, sqo, sqr,
    tksem, smsem, ldsem, gsR, grR, gsL, grL, sA, qA, sZ, qZ, sR, qR, hsR, hrR, hsL, hrL, sS, qS, rdyM, rdyZ,
):
    X = lax.axis_index("tp")
    Z = lax.axis_index("sp_0")
    Y = lax.axis_index("sp_1")
    C = lax.axis_index("sp_2")
    M = Y * NC + C
    right = lax.rem(X + 1, NX)
    left = lax.rem(X + NX - 1, NX)
    opp = lax.rem(X + 2, NX)

    def member(m):
        return {"sp_1": m // NC, "sp_2": lax.rem(m, NC)}

    late = jnp.where(Z == 0, NM - 1, 0)
    mine = lax.rem(M + late, NM)

    def load_rows(k):
        rows = pl.ds(k * Q, Q)
        return pltpu.make_async_copy(tokens.at[0, rows], xin.at[rows], tksem.at[k])

    small = [
        pltpu.make_async_copy(a, b, smsem.at[i])
        for i, (a, b) in enumerate(
            ((ing_in, ing), (slack_in, slack), (sud_in, sud), (hgain_in, hgain), (ogain_in, ogain))
        )
    ]
    loads = [pltpu.make_async_copy(w, W.at[i], ldsem.at[i]) for i, w in enumerate((wq, wf, wi, wg))]
    ld_wo = pltpu.make_async_copy(wo, WO, ldsem.at[4])
    small[0].start()
    for k in OUTER:
        load_rows(k).start()
    for c in small[1:]:
        c.start()
    for c in loads:
        c.start()
    ld_wo.start()

    barrier = pltpu.get_barrier_semaphore()
    for dx in range(1, NX):
        pl.semaphore_signal(barrier, inc=1, device_id={"tp": lax.rem(X + dx, NX)}, device_id_type=MESH)

    def greet_row(k, _):
        pl.semaphore_signal(barrier, inc=1, device_id=member(lax.rem(k + NM - late, NM)), device_id_type=MESH)
        return 0

    def greet_line(z, _):
        pl.semaphore_signal(barrier, inc=1, device_id={"sp_0": z}, device_id_type=MESH)
        return 0

    lax.fori_loop(mine + 1, NM, greet_row, 0)
    lax.fori_loop(Z + 1, NZ, greet_line, 0)

    small[0].wait()

    def norm_rows(k):
        def some(i, _):
            at = pl.ds(pl.multiple_of(k * Q + i * 16, 16), 16)
            rows = xin[at, :].astype(f32)
            rows = rows * lax.rsqrt(jnp.mean(rows * rows, axis=1, keepdims=True) + EPS) * ing[...]
            G[X, k, pl.ds(pl.multiple_of(i * 16, 16), 16), :] = rows.astype(bf16)
            return 0

        lax.fori_loop(0, Q // 16, some, 0)

    def to_right(who, k, slot):
        return pltpu.make_async_remote_copy(
            G.at[who, k], G.at[who, k], gsR.at[slot], grR.at[slot], device_id={"tp": right}, device_id_type=MESH
        )

    def to_left(who, k, slot):
        return pltpu.make_async_remote_copy(
            G.at[who, k], G.at[who, k], gsL.at[slot], grL.at[slot], device_id={"tp": left}, device_id_type=MESH
        )

    load_rows(0).wait()
    norm_rows(0)
    with jax.named_scope("barrier"):
        pl.semaphore_wait(barrier, (NX - 1) + mine + Z)
    to_right(X, 0, 0).start()
    load_rows(3).wait()
    norm_rows(3)
    to_left(X, 3, 3).start()
    load_rows(1).wait()
    norm_rows(1)
    to_right(X, 1, 1).start()
    load_rows(2).wait()
    norm_rows(2)
    to_left(X, 2, 2).start()
    to_right(X, 2, 2).start()
    to_left(X, 1, 1).start()
    to_right(X, 3, 3).start()
    to_left(X, 0, 0).start()

    def ready_row(k, _):
        pl.semaphore_signal(rdyM, inc=1, device_id=member(lax.rem(k + NM - late, NM)), device_id_type=MESH)
        return 0

    def ready_line(z, _):
        pl.semaphore_signal(rdyZ, inc=1, device_id={"sp_0": z}, device_id_type=MESH)
        return 0

    lax.fori_loop(0, mine, ready_row, 0)
    lax.fori_loop(0, Z, ready_line, 0)

    for c in small[1:]:
        c.wait()

    t_at = lax.broadcasted_iota(jnp.int32, (T, T), 0)
    s_at = lax.broadcasted_iota(jnp.int32, (T, T), 1)
    causal = s_at <= t_at
    tri = causal.astype(f32).astype(bf16)
    for b in range(NB):
        for h in range(2):
            line = jnp.broadcast_to(sud[h : h + 1, b * T : (b + 1) * T], (T, T))
            total = jnp.sum(jnp.where(causal, line, 0.0), axis=1, keepdims=True)
            BC[b, h] = jnp.broadcast_to(total, (T, T))

    with jax.named_scope("wload"):
        for c in loads:
            c.wait()

    def block_state(b):
        x = G[b].reshape(T, D)
        f_raw = dot(x, W[1]).astype(bf16).astype(f32)
        i_raw = dot(x, W[2]).astype(bf16)
        vv[b] = i_raw
        w = slack[...] * jax.nn.sigmoid(-f_raw)
        a = jnp.log1p(-w)
        a_hi = a.astype(bf16)
        a_lo = (a - a_hi.astype(f32)).astype(bf16)
        A = dot(tri, a_hi) + dot(tri, a_lo)
        AA[b] = A
        lk[b] = (w * jnp.exp(-A)).astype(bf16)
        for h in range(2):
            cols = slice(h * 128, (h + 1) * 128)
            reach = A[:, cols] + BC[b, h]
            end = reach[T - 1 : T, :]
            DT[b, h : h + 1, :] = end
            wk = (w[:, cols] * jnp.exp(end - reach)).astype(bf16)
            ST[b, h] = dot(i_raw[:, cols], wk, 0, 0)

    def block_rest(b):
        x = G[b].reshape(T, D)
        q_raw = dot(x, W[0]).astype(bf16).astype(f32) * KEY ** (-0.5)
        q_in = q_raw * jnp.exp(AA[b])
        lqA[b] = q_in.astype(bf16)
        for h in range(2):
            cols = slice(h * 128, (h + 1) * 128)
            lqD[b, :, cols] = q_in[:, cols] * jnp.exp(BC[b, h])
        g_raw = dot(x, W[3]).astype(bf16).astype(f32)
        silu = g_raw * jax.nn.sigmoid(g_raw)
        for h in range(2):
            cols = slice(h * 128, (h + 1) * 128)
            gs[b, :, cols] = silu[:, cols] * hgain[...]

    def arrive(i, _):
        @pl.when(i == 1)
        def _():
            with jax.named_scope("g1"):
                to_right(X, 0, 0).wait_recv()
                to_right(left, 0, 4).start()
                to_left(X, 3, 3).wait_recv()
                to_left(right, 3, 4).start()
                to_right(X, 1, 1).wait_recv()
                to_right(left, 1, 5).start()
                to_left(X, 2, 2).wait_recv()
                to_left(right, 2, 5).start()
            with jax.named_scope("g2"):
                for k in (2, 3):
                    to_right(X, k, k).wait_recv()
                    to_left(X, 3 - k, 3 - k).wait_recv()

        @pl.when(i == 3)
        def _():
            with jax.named_scope("g3"):
                to_right(left, 0, 4).wait_recv()
                to_left(right, 3, 4).wait_recv()
                to_right(left, 1, 5).wait_recv()
                to_left(right, 2, 5).wait_recv()

        b = lax.rem(X + 3 * i + 3 * (i // 2) + 2 * (i // 3), NX)
        with jax.named_scope("state"):
            block_state(b)

        @pl.when(i < 3)
        def _():
            with jax.named_scope("rest"):
                block_rest(b)

        return 0

    lax.fori_loop(0, NB, arrive, 0)

    finals, totals = [], []
    for h in range(2):
        state = jnp.zeros((128, 128), f32)
        reach = jnp.zeros((1, 128), f32)
        for b in range(NB):
            PB[b, h] = state.astype(bf16)
            DP[b, h : h + 1, :] = reach
            step = DT[b, h : h + 1, :]
            state = jnp.exp(step) * state + ST[b, h]
            reach = reach + step
        finals.append(state)
        totals.append(reach)
    for h in range(2):
        rows = decay_rows(totals[h])
        for j in range(NM // 2):
            m = h * (NM // 2) + j
            msgA[m, 0:PIECE, :] = finals[h][j * PIECE : (j + 1) * PIECE, :].astype(bf16)
            msgA[m, PIECE:MSG, :] = rows

    far_first = sorted(range(1, NM), key=lambda d: -min(d // 2, NY - d // 2))

    def piece_to(dm):
        m = lax.rem(M + dm, NM)
        return pltpu.make_async_remote_copy(
            msgA.at[m], rA.at[M], sA.at[dm], qA.at[dm], device_id=member(m), device_id_type=MESH
        )

    @pl.when(mine < NM - 1)
    def _():
        pl.semaphore_wait(rdyM, NM - 1 - mine)

    for dm in far_first:
        piece_to(dm).start()
    rA[M] = msgA[M]

    with jax.named_scope("rest3"):
        block_rest(opp)

    def inner(b, _):
        for h in range(2):
            cols = slice(h * 128, (h + 1) * 128)
            bc = BC[b, h]
            scores = dot(lqA[b, :, cols], lk[b, :, cols], 1, 1)
            scores = scores * jnp.exp(jnp.where(causal, bc - bc.T, -1e30))
            scores = jnp.where(causal, scores, 0.0)
            q_in = lqD[b, :, cols]
            O[b, :, cols] = dot(scores.astype(bf16), vv[b, :, cols]) + dot(q_in.astype(bf16), PB[b, h], 1, 1)
            lqA[b, :, cols] = (q_in * jnp.exp(DP[b, h : h + 1, :])).astype(bf16)
        return 0

    with jax.named_scope("inner"):
        lax.fori_loop(0, NB, inner, 0)

    with jax.named_scope("rswait"):
        for dm in range(1, NM):
            piece_to(dm).wait_recv()

    def decay_of(rows):
        part = rows[PIECE:MSG, :].astype(f32)
        return part[0:1, :] + part[1:2, :] + part[2:3, :]

    state = jnp.zeros((PIECE, 128), f32)
    reach = jnp.zeros((1, 128), f32)
    reaches = []
    for m in range(NM):
        rows = rA[m]
        Pp[m] = state
        reaches.append(reach)
        step = decay_of(rows)
        state = jnp.exp(step) * state + rows[0:PIECE, :].astype(f32)
        reach = reach + step
    zout[0:PIECE, :] = state.astype(bf16)
    zout[PIECE:MSG, :] = decay_rows(reach)

    def row_to(z):
        return pltpu.make_async_remote_copy(
            zout, rz.at[Z], sZ.at[z], qZ.at[Z], device_id={"sp_0": z}, device_id_type=MESH
        )

    def row_from(z):
        return pltpu.make_async_remote_copy(
            zout, rz.at[z], sZ.at[z], qZ.at[z], device_id={"sp_0": z}, device_id_type=MESH
        )

    def send_row(z, _):
        row_to(z).start()
        return 0

    @pl.when(Z < NZ - 1)
    def _():
        pl.semaphore_wait(rdyZ, NZ - 1 - Z)

    lax.fori_loop(Z + 1, NZ, send_row, 0)

    def take_row(z, before):
        row_from(z).wait_recv()
        rows = rz[z]
        return jnp.exp(decay_of(rows)) * before + rows[0:PIECE, :].astype(f32)

    with jax.named_scope("zwait"):
        before = lax.fori_loop(0, Z, take_row, jnp.zeros((PIECE, 128), f32))
    for m in range(NM):
        rout[m] = (jnp.exp(reaches[m]) * before + Pp[m]).astype(bf16)

    def back_to(dm):
        m = lax.rem(M + dm, NM)
        return pltpu.make_async_remote_copy(
            rout.at[m], SIN.at[M], sR.at[dm], qR.at[dm], device_id=member(m), device_id_type=MESH
        )

    for dm in far_first:
        back_to(dm).start()
    SIN[M] = rout[M]
    with jax.named_scope("backwait"):
        for dm in range(1, NM):
            back_to(dm).wait_recv()

    def h_right(who, r, half, slot):
        return pltpu.make_async_remote_copy(
            GG.at[who, r, half], GG.at[who, r, half], hsR.at[r, slot], hrR.at[r, slot],
            device_id={"tp": right}, device_id_type=MESH,
        )

    def h_left(who, r, half, slot):
        return pltpu.make_async_remote_copy(
            GG.at[who, r, half], GG.at[who, r, half], hsL.at[r, slot], hrL.at[r, slot],
            device_id={"tp": left}, device_id_type=MESH,
        )

    def readout(r, _):
        parts = []
        for h in range(2):
            cols = slice(h * 128, (h + 1) * 128)
            carried = SIN[h * 8 : (h + 1) * 8].reshape(128, 128)
            o = O[r, :, cols] + dot(lqA[r, :, cols], carried, 1, 1)
            o = o * lax.rsqrt(jnp.mean(o * o, axis=1, keepdims=True) + EPS)
            parts.append(o * gs[r, :, cols])
        gated = jnp.concatenate(parts, axis=1).astype(bf16)
        GG[X, r] = gated.reshape(2, H, W2)
        h_right(X, r, 0, 0).start()
        h_left(X, r, 1, 0).start()
        h_right(X, r, 1, 1).start()
        h_left(X, r, 0, 1).start()
        return 0

    with jax.named_scope("readout"):
        lax.fori_loop(0, NB, readout, 0)
        ld_wo.wait()

    def forward(r):
        h_right(X, r, 0, 0).wait_recv()
        h_right(left, r, 0, 2).start()
        h_left(X, r, 1, 0).wait_recv()
        h_left(right, r, 1, 2).start()

    def square_to(dx, r):
        return pltpu.make_async_remote_copy(
            sqo.at[r], sqr.at[dx - 1, r], sS.at[dx - 1, r], qS.at[dx - 1, r],
            device_id={"tp": lax.rem(X + dx, NX)}, device_id_type=MESH,
        )

    def project(r, _):
        @pl.when(r < NB - 1)
        def _():
            with jax.named_scope("hfwd"):
                forward(r + 1)

        with jax.named_scope("hwait"):
            h_right(X, r, 1, 1).wait_recv()
            h_left(X, r, 0, 1).wait_recv()
            h_right(left, r, 0, 2).wait_recv()
            h_left(right, r, 1, 2).wait_recv()
        acc = dot(GG[0, r].reshape(T, W2), WO[0:W2, :])
        for j in range(1, NX):
            acc = acc + dot(GG[j, r].reshape(T, W2), WO[j * W2 : (j + 1) * W2, :])
        PJ[r] = acc
        sq = acc * acc
        sq_hi = sq.astype(bf16)
        sq_lo = (sq - sq_hi.astype(f32)).astype(bf16)
        ones = jnp.ones((8, 512), f32).astype(bf16)
        sqo[r] = dot(ones, sq_hi, 1, 1) + dot(ones, sq_lo, 1, 1)
        for dx in (2, 1, 3):
            square_to(dx, r).start()
        return 0

    with jax.named_scope("hfwd0"):
        forward(0)
    lax.fori_loop(0, NB, project, 0)

    def finish(r, _):
        with jax.named_scope("sqwait"):
            for dx in (1, 2, 3):
                square_to(dx, r).wait_recv()
        total = sqo[r] + sqr[0, r] + sqr[1, r] + sqr[2, r]
        scale = lax.rsqrt(total[0:1, :] / D + EPS)
        scale = jnp.broadcast_to(scale, (T, T)).T
        for j in range(4):
            cols = slice(j * 128, (j + 1) * 128)
            out[0, pl.ds(pl.multiple_of(r * T, T), T), cols] = (
                PJ[r, :, cols] * scale * ogain[:, cols]
            ).astype(bf16)
        return 0

    lax.fori_loop(0, NB, finish, 0)

    for k in range(4):
        to_right(X, k, k).wait_send()
        to_left(X, k, k).wait_send()
    for k in range(2):
        to_right(left, k, 4 + k).wait_send()
        to_left(right, 3 - k, 4 + k).wait_send()
    for dm in range(1, NM):
        piece_to(dm).wait_send()
        back_to(dm).wait_send()

    def row_left(z, _):
        row_to(z).wait_send()
        return 0

    lax.fori_loop(Z + 1, NZ, row_left, 0)

    def rest(r, _):
        h_right(X, r, 0, 0).wait_send()
        h_right(X, r, 1, 1).wait_send()
        h_right(left, r, 0, 2).wait_send()
        h_left(X, r, 1, 0).wait_send()
        h_left(X, r, 0, 1).wait_send()
        h_left(right, r, 1, 2).wait_send()
        for dx in (1, 2, 3):
            square_to(dx, r).wait_send()
        return 0

    lax.fori_loop(0, NB, rest, 0)


def shards(tokens, ing, wq, wf, wi, wg, slack, sud, hgain, wo, ogain):
    vm = pl.BlockSpec(memory_space=pltpu.VMEM)
    hb = pl.BlockSpec(memory_space=pltpu.HBM)
    dma = pltpu.SemaphoreType.DMA
    V = pltpu.VMEM
    return pl.pallas_call(
        body,
        name="layer",
        out_shape=jax.ShapeDtypeStruct((1, 512, 512), bf16),
        in_specs=[hb] * 11,
        out_specs=vm,
        scratch_shapes=[
            V((1, D), f32), V((1, W2), f32), V((2, 512), f32), V((1, 128), f32), V((1, 512), f32),
            V((T, D), bf16),
            V((NX, 4, Q, D), bf16),
            V((4, D, W2), bf16),
            V((1024, 512), bf16),
            V((NB, T, W2), bf16),
            V((NB, T, W2), bf16),
            V((NB, T, W2), bf16),
            V((NB, T, W2), f32),
            V((NB, T, W2), f32),
            V((NB, 2, 128, 128), f32),
            V((NB, 2, 128, 128), bf16),
            V((NB, 2, 128), f32),
            V((NB, 2, 128), f32),
            V((NB, 2, T, T), f32),
            V((NX, T, W2), f32),
            V((NB, T, W2), f32),
            V((NM, MSG, 128), bf16),
            V((NM, MSG, 128), bf16),
            V((NM, PIECE, 128), f32),
            V((MSG, 128), bf16),
            V((NZ, MSG, 128), bf16),
            V((NM, PIECE, 128), bf16),
            V((NM, PIECE, 128), bf16),
            V((NX, NB, 2, H, W2), bf16),
            V((NB, T, 512), f32),
            V((NB, 8, 128), f32),
            V((3, NB, 8, 128), f32),
            dma((4,)), dma((5,)), dma((5,)),
            dma((6,)), dma((6,)), dma((6,)), dma((6,)),
            dma((NM,)), dma((NM,)),
            dma((NZ,)), dma((NZ,)),
            dma((NM,)), dma((NM,)),
            dma((NB, 3)), dma((NB, 3)), dma((NB, 3)), dma((NB, 3)),
            dma((3, NB)), dma((3, NB)),
            pltpu.SemaphoreType.REGULAR, pltpu.SemaphoreType.REGULAR,
        ],
        compiler_params=pltpu.CompilerParams(
            collective_id=0, has_side_effects=True, vmem_limit_bytes=60 * 1024 * 1024
        ),
    )(
        tokens,
        ing.reshape(1, D),
        wq, wf, wi, wg,
        slack.reshape(1, W2),
        sud[0].T,
        hgain.reshape(1, 128),
        wo,
        ogain.reshape(1, 512),
    )


def solution(mesh):
    torus = Mesh(mesh.devices.reshape(NZ, NY, NC, NX), ("sp_0", "sp_1", "sp_2", "tp"))
    in_specs = (
        P(None, SP_TP, None),
        P(),
        P(None, "tp"),
        P(None, "tp"),
        P(None, "tp"),
        P(None, "tp"),
        P("tp"),
        P(None, SP, "tp"),
        P(),
        P(None, "tp"),
        P("tp"),
    )
    out_specs = P(None, SP, "tp")
    return jax.shard_map(shards, mesh=torus, in_specs=in_specs, out_specs=out_specs, check_vma=False)
```

```python
import jax
import jax.numpy as jnp
from jax import lax
from jax.experimental import pallas as pl
from jax.experimental.pallas import tpu as pltpu
from jax.sharding import Mesh
from jax.sharding import PartitionSpec as P

D = 2048
KEY = 128
SP = ("sp_0", "sp_1", "sp_2")
SP_TP = ("sp_0", "sp_1", "sp_2", "tp")
MESH = pl.DeviceIdType.MESH
EPS = 1e-06

NZ, NY, NC, NX = 12, 8, 2, 4
NM = NY * NC
T = 128
H = T // 2
Q = T // 4
OUTER = (0, 3, 1, 2)
NB = 4
W2 = 256
NP = NY
PIECE = 256 // NP
MSG = PIECE + 8

bf16 = jnp.bfloat16
f32 = jnp.float32


def dot(a, b, ca=1, cb=0):
    return lax.dot_general(a, b, (((ca,), (cb,)), ((), ())), preferred_element_type=f32)


def split3(x):
    hi = x.astype(bf16).astype(f32)
    rest = x - hi
    mid = rest.astype(bf16).astype(f32)
    return hi, mid, rest - mid


def decay_rows(row):
    hi, mid, lo = split3(row)
    at = lax.broadcasted_iota(jnp.int32, (8, 128), 0)
    rows = jnp.where(at == 0, hi, jnp.where(at == 1, mid, jnp.where(at == 2, lo, 0.0)))
    return rows.astype(bf16)


def body(
    tokens, ing_in, wq, wf, wi, wg, slack_in, sud_in, hgain_in, wo, ogain_in, out,
    ing, slack, sud, hgain, ogain,
    xin, G, W, WO, lqA, lk, vv, lqD, gs, ST, PB, DT, DP, BC, AA, O,
    msgA, rA, Pp, zout, rz, rout, SIN, GG, PJ, sqo, sqr,
    tksem, smsem, ldsem, gsR, grR, gsL, grL, sA, qA, sZ, qZ, sR, qR, hsR, hrR, hsL, hrL, sS, qS, rdyM, rdyZ,
):
    X = lax.axis_index("tp")
    Z = lax.axis_index("sp_0")
    Y = lax.axis_index("sp_1")
    C = lax.axis_index("sp_2")
    M = Y * NC + C
    right = lax.rem(X + 1, NX)
    left = lax.rem(X + NX - 1, NX)
    opp = lax.rem(X + 2, NX)

    def member(m):
        return {"sp_1": m // NC, "sp_2": lax.rem(m, NC)}

    late = jnp.where(Z == 0, NM - 1, 0)
    mine = lax.rem(M + late, NM)

    barrier = pltpu.get_barrier_semaphore()
    for dx in range(1, NX):
        pl.semaphore_signal(barrier, inc=1, device_id={"tp": lax.rem(X + dx, NX)}, device_id_type=MESH)

    def load_rows(k):
        rows = pl.ds(k * Q, Q)
        return pltpu.make_async_copy(tokens.at[0, rows], xin.at[rows], tksem.at[k])

    small = [
        pltpu.make_async_copy(a, b, smsem.at[i])
        for i, (a, b) in enumerate(
            ((ing_in, ing), (slack_in, slack), (sud_in, sud), (hgain_in, hgain), (ogain_in, ogain))
        )
    ]
    loads = [pltpu.make_async_copy(w, W.at[i], ldsem.at[i]) for i, w in enumerate((wq, wf, wi, wg))]
    ld_wo = pltpu.make_async_copy(wo, WO, ldsem.at[4])
    small[0].start()
    for k in OUTER:
        load_rows(k).start()
    for c in small[1:]:
        c.start()
    for c in loads:
        c.start()
    ld_wo.start()

    def greet_row(k, _):
        pl.semaphore_signal(barrier, inc=1, device_id=member(lax.rem(k + NM - late, NM)), device_id_type=MESH)
        return 0

    def greet_line(z, _):
        pl.semaphore_signal(barrier, inc=1, device_id={"sp_0": z}, device_id_type=MESH)
        return 0

    lax.fori_loop(mine + 1, NM, greet_row, 0)

    @pl.when(C == 1)
    def _():
        lax.fori_loop(Z + 1, NZ, greet_line, 0)


    small[0].wait()

    def norm_rows(k):
        def some(i, _):
            at = pl.ds(pl.multiple_of(k * Q + i * 16, 16), 16)
            rows = xin[at, :].astype(f32)
            rows = rows * lax.rsqrt(jnp.mean(rows * rows, axis=1, keepdims=True) + EPS) * ing[...]
            G[X, k, pl.ds(pl.multiple_of(i * 16, 16), 16), :] = rows.astype(bf16)
            return 0

        lax.fori_loop(0, Q // 16, some, 0)

    def to_right(who, k, slot):
        return pltpu.make_async_remote_copy(
            G.at[who, k], G.at[who, k], gsR.at[slot], grR.at[slot], device_id={"tp": right}, device_id_type=MESH
        )

    def to_left(who, k, slot):
        return pltpu.make_async_remote_copy(
            G.at[who, k], G.at[who, k], gsL.at[slot], grL.at[slot], device_id={"tp": left}, device_id_type=MESH
        )

    load_rows(0).wait()
    norm_rows(0)
    with jax.named_scope("barrier"):
        pl.semaphore_wait(barrier, (NX - 1) + mine + Z * C)
    to_right(X, 0, 0).start()
    load_rows(3).wait()
    norm_rows(3)
    to_left(X, 3, 3).start()
    load_rows(1).wait()
    norm_rows(1)
    to_right(X, 1, 1).start()
    load_rows(2).wait()
    norm_rows(2)
    to_left(X, 2, 2).start()
    to_right(X, 2, 2).start()
    to_left(X, 1, 1).start()
    to_right(X, 3, 3).start()
    to_left(X, 0, 0).start()

    def ready_row(k, _):
        pl.semaphore_signal(rdyM, inc=1, device_id=member(lax.rem(k + NM - late, NM)), device_id_type=MESH)
        return 0

    def ready_line(z, _):
        pl.semaphore_signal(rdyZ, inc=1, device_id={"sp_0": z}, device_id_type=MESH)
        return 0

    lax.fori_loop(0, mine, ready_row, 0)

    @pl.when(C == 1)
    def _():
        lax.fori_loop(0, Z, ready_line, 0)


    for c in small[1:]:
        c.wait()

    t_at = lax.broadcasted_iota(jnp.int32, (T, T), 0)
    s_at = lax.broadcasted_iota(jnp.int32, (T, T), 1)
    causal = s_at <= t_at
    tri = causal.astype(f32).astype(bf16)
    for b in range(NB):
        for h in range(2):
            line = jnp.broadcast_to(sud[h : h + 1, b * T : (b + 1) * T], (T, T))
            total = jnp.sum(jnp.where(causal, line, 0.0), axis=1, keepdims=True)
            BC[b, h] = jnp.broadcast_to(total, (T, T))

    with jax.named_scope("wload"):
        for c in loads:
            c.wait()

    def block_state(b):
        x = G[b].reshape(T, D)
        f_raw = dot(x, W[1]).astype(bf16).astype(f32)
        i_raw = dot(x, W[2]).astype(bf16)
        vv[b] = i_raw
        w = slack[...] * jax.nn.sigmoid(-f_raw)
        a = jnp.log1p(-w)
        a_hi = a.astype(bf16)
        a_lo = (a - a_hi.astype(f32)).astype(bf16)
        A = dot(tri, a_hi) + dot(tri, a_lo)
        AA[b] = A
        lk[b] = (w * jnp.exp(-A)).astype(bf16)
        for h in range(2):
            cols = slice(h * 128, (h + 1) * 128)
            reach = A[:, cols] + BC[b, h]
            end = reach[T - 1 : T, :]
            DT[b, h : h + 1, :] = end
            wk = (w[:, cols] * jnp.exp(end - reach)).astype(bf16)
            ST[b, h] = dot(i_raw[:, cols], wk, 0, 0)

    def block_rest(b):
        x = G[b].reshape(T, D)
        q_raw = dot(x, W[0]).astype(bf16).astype(f32) * KEY ** (-0.5)
        q_in = q_raw * jnp.exp(AA[b])
        lqA[b] = q_in.astype(bf16)
        for h in range(2):
            cols = slice(h * 128, (h + 1) * 128)
            lqD[b, :, cols] = q_in[:, cols] * jnp.exp(BC[b, h])
        g_raw = dot(x, W[3]).astype(bf16).astype(f32)
        silu = g_raw * jax.nn.sigmoid(g_raw)
        for h in range(2):
            cols = slice(h * 128, (h + 1) * 128)
            gs[b, :, cols] = silu[:, cols] * hgain[...]

    def arrive(i, _):
        @pl.when(i == 1)
        def _():
            with jax.named_scope("g1"):
                to_right(X, 0, 0).wait_recv()
                to_right(left, 0, 4).start()
                to_left(X, 3, 3).wait_recv()
                to_left(right, 3, 4).start()
                to_right(X, 1, 1).wait_recv()
                to_right(left, 1, 5).start()
                to_left(X, 2, 2).wait_recv()
                to_left(right, 2, 5).start()
            with jax.named_scope("g2"):
                for k in (2, 3):
                    to_right(X, k, k).wait_recv()
                    to_left(X, 3 - k, 3 - k).wait_recv()

        @pl.when(i == 3)
        def _():
            with jax.named_scope("g3"):
                to_right(left, 0, 4).wait_recv()
                to_left(right, 3, 4).wait_recv()
                to_right(left, 1, 5).wait_recv()
                to_left(right, 2, 5).wait_recv()

        b = lax.rem(X + 3 * i + 3 * (i // 2) + 2 * (i // 3), NX)
        with jax.named_scope("state"):
            block_state(b)

        @pl.when(i < 3)
        def _():
            with jax.named_scope("rest"):
                block_rest(b)

        return 0

    lax.fori_loop(0, NB, arrive, 0)

    finals, totals = [], []
    for h in range(2):
        state = jnp.zeros((128, 128), f32)
        reach = jnp.zeros((1, 128), f32)
        for b in range(NB):
            PB[b, h] = state.astype(bf16)
            DP[b, h : h + 1, :] = reach
            step = DT[b, h : h + 1, :]
            state = jnp.exp(step) * state + ST[b, h]
            reach = reach + step
        finals.append(state)
        totals.append(reach)
    for h in range(2):
        rows = decay_rows(totals[h])
        for j in range(NP // 2):
            p = h * (NP // 2) + j
            msgA[p, 0:PIECE, :] = finals[h][j * PIECE : (j + 1) * PIECE, :].astype(bf16)
            msgA[p, PIECE:MSG, :] = rows

    far_first = sorted(range(NP), key=lambda d: -min(d, NP - d))

    def piece_to(dy):
        p = lax.rem(Y + dy, NP)
        at = 2 * dy + 1 - C
        return pltpu.make_async_remote_copy(
            msgA.at[p], rA.at[M], sA.at[dy], qA.at[at], device_id={"sp_1": p, "sp_2": 1}, device_id_type=MESH
        )

    def piece_from(at):
        return pltpu.make_async_remote_copy(
            msgA.at[0], rA.at[M], sA.at[0], qA.at[at], device_id={"sp_1": Y, "sp_2": 1}, device_id_type=MESH
        )

    @pl.when(mine < NM - 1)
    def _():
        pl.semaphore_wait(rdyM, NM - 1 - mine)

    for dy in far_first[:-1]:
        piece_to(dy).start()

    @pl.when(C == 0)
    def _():
        piece_to(0).start()

    @pl.when(C == 1)
    def _():
        rA[M] = msgA[Y]

    with jax.named_scope("rest3"):
        block_rest(opp)

    def inner(b, _):
        for h in range(2):
            cols = slice(h * 128, (h + 1) * 128)
            bc = BC[b, h]
            scores = dot(lqA[b, :, cols], lk[b, :, cols], 1, 1)
            scores = scores * jnp.exp(jnp.where(causal, bc - bc.T, -1e30))
            scores = jnp.where(causal, scores, 0.0)
            q_in = lqD[b, :, cols]
            O[b, :, cols] = dot(scores.astype(bf16), vv[b, :, cols]) + dot(q_in.astype(bf16), PB[b, h], 1, 1)
            lqA[b, :, cols] = (q_in * jnp.exp(DP[b, h : h + 1, :])).astype(bf16)
        return 0

    with jax.named_scope("inner"):
        lax.fori_loop(0, NB, inner, 0)

    def decay_of(rows):
        part = rows[PIECE:MSG, :].astype(f32)
        return part[0:1, :] + part[1:2, :] + part[2:3, :]

    def row_to(z):
        return pltpu.make_async_remote_copy(
            zout, rz.at[Z], sZ.at[z], qZ.at[Z], device_id={"sp_0": z}, device_id_type=MESH
        )

    def row_from(z):
        return pltpu.make_async_remote_copy(
            zout, rz.at[z], sZ.at[z], qZ.at[z], device_id={"sp_0": z}, device_id_type=MESH
        )

    def send_row(z, _):
        row_to(z).start()
        return 0

    def take_row(z, before):
        row_from(z).wait_recv()
        rows = rz[z]
        return jnp.exp(decay_of(rows)) * before + rows[0:PIECE, :].astype(f32)

    def back_to(dm):
        m = lax.rem(M + dm, NM)
        return pltpu.make_async_remote_copy(
            rout.at[m], SIN.at[Y], sR.at[dm], qR.at[Y], device_id=member(m), device_id_type=MESH
        )

    def back_from(dy):
        p = lax.rem(Y + dy, NP)
        return pltpu.make_async_remote_copy(
            rout.at[0], SIN.at[p], sR.at[0], qR.at[p], device_id={"sp_1": p, "sp_2": 1}, device_id_type=MESH
        )

    back_order = sorted(range(1, NM), key=lambda d: -min(d // 2, NY - d // 2))

    @pl.when(C == 1)
    def _():
        with jax.named_scope("rswait"):
            for at in range(1, NM):
                piece_from(at).wait_recv()

        state = jnp.zeros((PIECE, 128), f32)
        reach = jnp.zeros((1, 128), f32)
        reaches = []
        for m in range(NM):
            rows = rA[m]
            Pp[m] = state
            reaches.append(reach)
            step = decay_of(rows)
            state = jnp.exp(step) * state + rows[0:PIECE, :].astype(f32)
            reach = reach + step
        zout[0:PIECE, :] = state.astype(bf16)
        zout[PIECE:MSG, :] = decay_rows(reach)

        @pl.when(Z < NZ - 1)
        def _():
            pl.semaphore_wait(rdyZ, NZ - 1 - Z)

        lax.fori_loop(Z + 1, NZ, send_row, 0)
        with jax.named_scope("zwait"):
            before = lax.fori_loop(0, Z, take_row, jnp.zeros((PIECE, 128), f32))
        for m in range(NM):
            rout[m] = (jnp.exp(reaches[m]) * before + Pp[m]).astype(bf16)
        for dm in back_order:
            back_to(dm).start()
        SIN[Y] = rout[M]

    with jax.named_scope("backwait"):
        for dy in far_first[:-1]:
            back_from(dy).wait_recv()

        @pl.when(C == 0)
        def _():
            back_from(0).wait_recv()

    def h_right(who, r, half, slot):
        return pltpu.make_async_remote_copy(
            GG.at[who, r, half], GG.at[who, r, half], hsR.at[r, slot], hrR.at[r, slot],
            device_id={"tp": right}, device_id_type=MESH,
        )

    def h_left(who, r, half, slot):
        return pltpu.make_async_remote_copy(
            GG.at[who, r, half], GG.at[who, r, half], hsL.at[r, slot], hrL.at[r, slot],
            device_id={"tp": left}, device_id_type=MESH,
        )

    def readout(r, _):
        parts = []
        for h in range(2):
            cols = slice(h * 128, (h + 1) * 128)
            carried = SIN[h * (NP // 2) : (h + 1) * (NP // 2)].reshape(128, 128)
            o = O[r, :, cols] + dot(lqA[r, :, cols], carried, 1, 1)
            o = o * lax.rsqrt(jnp.mean(o * o, axis=1, keepdims=True) + EPS)
            parts.append(o * gs[r, :, cols])
        gated = jnp.concatenate(parts, axis=1).astype(bf16)
        GG[X, r] = gated.reshape(2, H, W2)
        h_right(X, r, 0, 0).start()
        h_left(X, r, 1, 0).start()
        h_right(X, r, 1, 1).start()
        h_left(X, r, 0, 1).start()
        return 0

    with jax.named_scope("readout"):
        lax.fori_loop(0, NB, readout, 0)
        ld_wo.wait()

    def forward(r):
        h_right(X, r, 0, 0).wait_recv()
        h_right(left, r, 0, 2).start()
        h_left(X, r, 1, 0).wait_recv()
        h_left(right, r, 1, 2).start()

    def square_to(dx, r):
        return pltpu.make_async_remote_copy(
            sqo.at[r], sqr.at[dx - 1, r], sS.at[dx - 1, r], qS.at[dx - 1, r],
            device_id={"tp": lax.rem(X + dx, NX)}, device_id_type=MESH,
        )

    for r in range(NB):
        with jax.named_scope("hfwd"):
            forward(r)

    def near(r, _):
        with jax.named_scope("hnear"):
            h_right(X, r, 1, 1).wait_recv()
            h_left(X, r, 0, 1).wait_recv()
        acc = dot(GG[X, r].reshape(T, W2), WO[X])
        acc = acc + dot(GG[left, r].reshape(T, W2), WO[left])
        PJ[r] = acc + dot(GG[right, r].reshape(T, W2), WO[right])
        return 0

    lax.fori_loop(0, NB, near, 0)

    def far(r, _):
        with jax.named_scope("hfar"):
            h_right(left, r, 0, 2).wait_recv()
            h_left(right, r, 1, 2).wait_recv()
        acc = PJ[r] + dot(GG[opp, r].reshape(T, W2), WO[opp])
        PJ[r] = acc
        sq = acc * acc
        sq_hi = sq.astype(bf16)
        sq_lo = (sq - sq_hi.astype(f32)).astype(bf16)
        ones = jnp.ones((8, 512), f32).astype(bf16)
        sqo[r] = dot(ones, sq_hi, 1, 1) + dot(ones, sq_lo, 1, 1)
        for dx in (2, 1, 3):
            square_to(dx, r).start()
        return 0

    lax.fori_loop(0, NB, far, 0)

    def finish(r, _):
        with jax.named_scope("sqwait"):
            for dx in (1, 2, 3):
                square_to(dx, r).wait_recv()
        total = sqo[r] + sqr[0, r] + sqr[1, r] + sqr[2, r]
        scale = lax.rsqrt(total[0:1, :] / D + EPS)
        scale = jnp.broadcast_to(scale, (T, T)).T
        for j in range(4):
            cols = slice(j * 128, (j + 1) * 128)
            out[0, pl.ds(pl.multiple_of(r * T, T), T), cols] = (
                PJ[r, :, cols] * scale * ogain[:, cols]
            ).astype(bf16)
        return 0

    lax.fori_loop(0, NB, finish, 0)

    for k in range(4):
        to_right(X, k, k).wait_send()
        to_left(X, k, k).wait_send()
    for k in range(2):
        to_right(left, k, 4 + k).wait_send()
        to_left(right, 3 - k, 4 + k).wait_send()
    for dy in range(1, NP):
        piece_to(dy).wait_send()

    @pl.when(C == 0)
    def _():
        piece_to(0).wait_send()

    def row_left(z, _):
        row_to(z).wait_send()
        return 0

    @pl.when(C == 1)
    def _():
        for dm in range(1, NM):
            back_to(dm).wait_send()
        lax.fori_loop(Z + 1, NZ, row_left, 0)

    def rest(r, _):
        h_right(X, r, 0, 0).wait_send()
        h_right(X, r, 1, 1).wait_send()
        h_right(left, r, 0, 2).wait_send()
        h_left(X, r, 1, 0).wait_send()
        h_left(X, r, 0, 1).wait_send()
        h_left(right, r, 1, 2).wait_send()
        for dx in (1, 2, 3):
            square_to(dx, r).wait_send()
        return 0

    lax.fori_loop(0, NB, rest, 0)


def shards(tokens, ing, wq, wf, wi, wg, slack, sud, hgain, wo, ogain):
    vm = pl.BlockSpec(memory_space=pltpu.VMEM)
    hb = pl.BlockSpec(memory_space=pltpu.HBM)
    dma = pltpu.SemaphoreType.DMA
    V = pltpu.VMEM
    return pl.pallas_call(
        body,
        name="layer",
        out_shape=jax.ShapeDtypeStruct((1, 512, 512), bf16),
        in_specs=[hb] * 11,
        out_specs=vm,
        scratch_shapes=[
            V((1, D), f32), V((1, W2), f32), V((2, 512), f32), V((1, 128), f32), V((1, 512), f32),
            V((T, D), bf16),
            V((NX, 4, Q, D), bf16),
            V((4, D, W2), bf16),
            V((NX, W2, 512), bf16),
            V((NB, T, W2), bf16),
            V((NB, T, W2), bf16),
            V((NB, T, W2), bf16),
            V((NB, T, W2), f32),
            V((NB, T, W2), f32),
            V((NB, 2, 128, 128), f32),
            V((NB, 2, 128, 128), bf16),
            V((NB, 2, 128), f32),
            V((NB, 2, 128), f32),
            V((NB, 2, T, T), f32),
            V((NX, T, W2), f32),
            V((NB, T, W2), f32),
            V((NP, MSG, 128), bf16),
            V((NM, MSG, 128), bf16),
            V((NM, PIECE, 128), f32),
            V((MSG, 128), bf16),
            V((NZ, MSG, 128), bf16),
            V((NM, PIECE, 128), bf16),
            V((NP, PIECE, 128), bf16),
            V((NX, NB, 2, H, W2), bf16),
            V((NB, T, 512), f32),
            V((NB, 8, 128), f32),
            V((3, NB, 8, 128), f32),
            dma((4,)), dma((5,)), dma((5,)),
            dma((6,)), dma((6,)), dma((6,)), dma((6,)),
            dma((NP,)), dma((NM,)),
            dma((NZ,)), dma((NZ,)),
            dma((NM,)), dma((NP,)),
            dma((NB, 3)), dma((NB, 3)), dma((NB, 3)), dma((NB, 3)),
            dma((3, NB)), dma((3, NB)),
            pltpu.SemaphoreType.REGULAR, pltpu.SemaphoreType.REGULAR,
        ],
        compiler_params=pltpu.CompilerParams(
            collective_id=0, has_side_effects=True, vmem_limit_bytes=40 * 1024 * 1024
        ),
    )(
        *(
            pltpu.with_memory_space_constraint(x, pltpu.HBM)
            for x in (
                tokens,
                ing.reshape(1, D),
                wq, wf, wi, wg,
                slack.reshape(1, W2),
                sud[0].T,
                hgain.reshape(1, 128),
                wo.reshape(NX, W2, 512),
                ogain.reshape(1, 512),
            )
        )
    )


def solution(mesh):
    torus = Mesh(mesh.devices.reshape(NZ, NY, NC, NX), ("sp_0", "sp_1", "sp_2", "tp"))
    in_specs = (
        P(None, SP_TP, None),
        P(),
        P(None, "tp"),
        P(None, "tp"),
        P(None, "tp"),
        P(None, "tp"),
        P("tp"),
        P(None, SP, "tp"),
        P(),
        P(None, "tp"),
        P("tp"),
    )
    out_specs = P(None, SP, "tp")
    return jax.shard_map(shards, mesh=torus, in_specs=in_specs, out_specs=out_specs, check_vma=False)
```

```python
import jax
import jax.numpy as jnp
from jax import lax
from jax.experimental import pallas as pl
from jax.experimental.pallas import tpu as pltpu
from jax.sharding import Mesh
from jax.sharding import PartitionSpec as P

D = 2048
KEY = 128
SP = ("sp_0", "sp_1", "sp_2")
SP_TP = ("sp_0", "sp_1", "sp_2", "tp")
MESH = pl.DeviceIdType.MESH
EPS = 1e-06

NZ, NY, NC, NX = 12, 8, 2, 4
NM = NY * NC
T = 128
H = T // 2
Q = T // 4
OUTER = (0, 3, 1, 2)
NB = 4
W2 = 256
NP = NY
PIECE = 256 // NP
MSG = PIECE + 8

bf16 = jnp.bfloat16
f32 = jnp.float32


def dot(a, b, ca=1, cb=0):
    return lax.dot_general(a, b, (((ca,), (cb,)), ((), ())), preferred_element_type=f32)


def split3(x):
    hi = x.astype(bf16).astype(f32)
    rest = x - hi
    mid = rest.astype(bf16).astype(f32)
    return hi, mid, rest - mid


def decay_rows(row):
    hi, mid, lo = split3(row)
    at = lax.broadcasted_iota(jnp.int32, (8, 128), 0)
    rows = jnp.where(at == 0, hi, jnp.where(at == 1, mid, jnp.where(at == 2, lo, 0.0)))
    return rows.astype(bf16)


def body(
    tokens, ing_in, wq, wf, wi, wg, slack_in, sud_in, hgain_in, wo, ogain_in, out,
    ing, slack, sud, hgain, ogain,
    xin, G, W, WO, lqA, lk, vv, lqD, gs, ST, PB, DT, DP, BC, AA, O,
    msgA, rA, Pp, zout, rz, rout, SIN, GG, PJ, sqo, sqr,
    tksem, smsem, ldsem, gsR, grR, gsL, grL, sA, qA, sZ, qZ, sR, qR, hsR, hrR, hsL, hrL, sS, qS, rdyM, rdyZ,
):
    X = lax.axis_index("tp")
    Z = lax.axis_index("sp_0")
    Y = lax.axis_index("sp_1")
    C = lax.axis_index("sp_2")
    M = Y * NC + C
    right = lax.rem(X + 1, NX)
    left = lax.rem(X + NX - 1, NX)
    opp = lax.rem(X + 2, NX)

    def member(m):
        return {"sp_1": m // NC, "sp_2": lax.rem(m, NC)}

    host_y = jnp.where(Z == 0, 0, NY // 2)
    host_c = jnp.where(Z == 0, 0, 1)
    hosts_row = (Y == host_y) & (C == host_c)
    hosts_line = (Z == NZ - 1) & (C == 1)
    host = host_y * NC + host_c
    to_hear = 2 + jnp.where(hosts_row, NM - 1, 0) + jnp.where(hosts_line, NZ - 1, 0)
    barrier = pltpu.get_barrier_semaphore()

    def load_rows(k):
        rows = pl.ds(k * Q, Q)
        return pltpu.make_async_copy(tokens.at[0, rows], xin.at[rows], tksem.at[k])

    small = [
        pltpu.make_async_copy(a, b, smsem.at[i])
        for i, (a, b) in enumerate(
            ((ing_in, ing), (slack_in, slack), (sud_in, sud), (hgain_in, hgain), (ogain_in, ogain))
        )
    ]
    loads = [pltpu.make_async_copy(w, W.at[i], ldsem.at[i]) for i, w in enumerate((wq, wf, wi, wg))]
    ld_wo = pltpu.make_async_copy(wo, WO, ldsem.at[4])
    load_rows(0).start()
    small[0].start()
    for side in (right, left):
        pl.semaphore_signal(barrier, inc=1, device_id={"tp": side}, device_id_type=MESH)
    for k in OUTER[1:]:
        load_rows(k).start()

    @pl.when(jnp.logical_not(hosts_row))
    def _():
        pl.semaphore_signal(barrier, inc=1, device_id={"sp_1": host_y, "sp_2": host_c}, device_id_type=MESH)

    @pl.when((Z < NZ - 1) & (C == 1))
    def _():
        pl.semaphore_signal(barrier, inc=1, device_id={"sp_0": NZ - 1}, device_id_type=MESH)

    small[0].wait()

    def norm_rows(k):
        def some(i, _):
            at = pl.ds(pl.multiple_of(k * Q + i * 16, 16), 16)
            rows = xin[at, :].astype(f32)
            rows = rows * lax.rsqrt(jnp.mean(rows * rows, axis=1, keepdims=True) + EPS) * ing[...]
            G[X, k, pl.ds(pl.multiple_of(i * 16, 16), 16), :] = rows.astype(bf16)
            return 0

        lax.fori_loop(0, Q // 16, some, 0)

    def to_right(who, k, slot):
        return pltpu.make_async_remote_copy(
            G.at[who, k], G.at[who, k], gsR.at[slot // 4], grR.at[slot], device_id={"tp": right}, device_id_type=MESH
        )

    def to_left(who, k, slot):
        return pltpu.make_async_remote_copy(
            G.at[who, k], G.at[who, k], gsL.at[slot // 4], grL.at[slot], device_id={"tp": left}, device_id_type=MESH
        )

    with jax.named_scope("ld0"):
        load_rows(0).wait()
    with jax.named_scope("n0"):
        norm_rows(0)
        load_rows(3).wait()
        norm_rows(3)
    with jax.named_scope("barrier"):
        pl.semaphore_wait(barrier, to_hear)
    to_right(X, 0, 0).start()
    to_left(X, 3, 3).start()
    for c in loads:
        c.start()
    for c in small[1:]:
        c.start()
    ld_wo.start()
    load_rows(1).wait()
    norm_rows(1)
    to_right(X, 1, 1).start()
    load_rows(2).wait()
    norm_rows(2)
    to_left(X, 2, 2).start()
    to_right(X, 2, 2).start()
    to_left(X, 1, 1).start()
    to_right(X, 3, 3).start()
    to_left(X, 0, 0).start()

    def ready_row(k, _):
        pl.semaphore_signal(rdyM, inc=1, device_id=member(lax.rem(host + k, NM)), device_id_type=MESH)
        return 0

    def ready_line(z, _):
        pl.semaphore_signal(rdyZ, inc=1, device_id={"sp_0": z}, device_id_type=MESH)
        return 0

    @pl.when(hosts_row)
    def _():
        lax.fori_loop(1, NM, ready_row, 0)

    @pl.when(hosts_line)
    def _():
        lax.fori_loop(0, NZ - 1, ready_line, 0)

    for c in small[1:]:
        c.wait()

    t_at = lax.broadcasted_iota(jnp.int32, (T, T), 0)
    s_at = lax.broadcasted_iota(jnp.int32, (T, T), 1)
    causal = s_at <= t_at
    tri = causal.astype(f32).astype(bf16)
    for b in range(NB):
        for h in range(2):
            line = jnp.broadcast_to(sud[h : h + 1, b * T : (b + 1) * T], (T, T))
            total = jnp.sum(jnp.where(causal, line, 0.0), axis=1, keepdims=True)
            BC[b, h] = jnp.broadcast_to(total, (T, T))

    with jax.named_scope("wload"):
        for c in loads:
            c.wait()

    def block_state(b):
        x = G[b].reshape(T, D)
        f_raw = dot(x, W[1]).astype(bf16).astype(f32)
        i_raw = dot(x, W[2]).astype(bf16)
        vv[b] = i_raw
        w = slack[...] * jax.nn.sigmoid(-f_raw)
        a = jnp.log1p(-w)
        a_hi = a.astype(bf16)
        a_lo = (a - a_hi.astype(f32)).astype(bf16)
        A = dot(tri, a_hi) + dot(tri, a_lo)
        AA[b] = A
        lk[b] = (w * jnp.exp(-A)).astype(bf16)
        for h in range(2):
            cols = slice(h * 128, (h + 1) * 128)
            reach = A[:, cols] + BC[b, h]
            end = reach[T - 1 : T, :]
            DT[b, h : h + 1, :] = end
            wk = (w[:, cols] * jnp.exp(end - reach)).astype(bf16)
            ST[b, h] = dot(i_raw[:, cols], wk, 0, 0)

    def block_rest(b):
        x = G[b].reshape(T, D)
        q_raw = dot(x, W[0]).astype(bf16).astype(f32) * KEY ** (-0.5)
        q_in = q_raw * jnp.exp(AA[b])
        lqA[b] = q_in.astype(bf16)
        for h in range(2):
            cols = slice(h * 128, (h + 1) * 128)
            lqD[b, :, cols] = q_in[:, cols] * jnp.exp(BC[b, h])
        g_raw = dot(x, W[3]).astype(bf16).astype(f32)
        silu = g_raw * jax.nn.sigmoid(g_raw)
        for h in range(2):
            cols = slice(h * 128, (h + 1) * 128)
            gs[b, :, cols] = silu[:, cols] * hgain[...]

    def arrive(i, _):
        @pl.when(i == 1)
        def _():
            with jax.named_scope("g1"):
                to_right(X, 0, 0).wait_recv()
                to_right(left, 0, 4).start()
                to_left(X, 3, 3).wait_recv()
                to_left(right, 3, 4).start()
                to_right(X, 1, 1).wait_recv()
                to_right(left, 1, 5).start()
                to_left(X, 2, 2).wait_recv()
                to_left(right, 2, 5).start()
            with jax.named_scope("g2"):
                for k in (2, 3):
                    to_right(X, k, k).wait_recv()
                    to_left(X, 3 - k, 3 - k).wait_recv()

        @pl.when(i == 3)
        def _():
            with jax.named_scope("g3"):
                to_right(left, 0, 4).wait_recv()
                to_left(right, 3, 4).wait_recv()
                to_right(left, 1, 5).wait_recv()
                to_left(right, 2, 5).wait_recv()

        b = lax.rem(X + 3 * i + 3 * (i // 2) + 2 * (i // 3), NX)
        with jax.named_scope("state"):
            block_state(b)

        @pl.when(i < 3)
        def _():
            with jax.named_scope("rest"):
                block_rest(b)

        return 0

    lax.fori_loop(0, NB, arrive, 0)

    finals, totals = [], []
    for h in range(2):
        state = jnp.zeros((128, 128), f32)
        reach = jnp.zeros((1, 128), f32)
        for b in range(NB):
            PB[b, h] = state.astype(bf16)
            DP[b, h : h + 1, :] = reach
            step = DT[b, h : h + 1, :]
            state = jnp.exp(step) * state + ST[b, h]
            reach = reach + step
        finals.append(state)
        totals.append(reach)
    for h in range(2):
        rows = decay_rows(totals[h])
        for j in range(NP // 2):
            p = h * (NP // 2) + j
            msgA[p, 0:PIECE, :] = finals[h][j * PIECE : (j + 1) * PIECE, :].astype(bf16)
            msgA[p, PIECE:MSG, :] = rows

    far_first = sorted(range(NP), key=lambda d: -min(d, NP - d))

    def piece_to(dy):
        p = lax.rem(Y + dy, NP)
        return pltpu.make_async_remote_copy(
            msgA.at[p], rA.at[M], sA, qA, device_id={"sp_1": p, "sp_2": 1}, device_id_type=MESH
        )

    @pl.when(jnp.logical_not(hosts_row))
    def _():
        pl.semaphore_wait(rdyM, 1)

    for dy in far_first[:-1]:
        piece_to(dy).start()

    @pl.when(C == 0)
    def _():
        piece_to(0).start()

    @pl.when(C == 1)
    def _():
        rA[M] = msgA[Y]

    for sem, near_one in ((gsR, left), (gsL, right)):
        pltpu.make_async_copy(G.at[X], G.at[X], sem.at[0]).wait()
        pltpu.make_async_copy(G.at[near_one, 0:2], G.at[near_one, 0:2], sem.at[1]).wait()

    with jax.named_scope("rest3"):
        block_rest(opp)

    def inner(b, _):
        for h in range(2):
            cols = slice(h * 128, (h + 1) * 128)
            bc = BC[b, h]
            scores = dot(lqA[b, :, cols], lk[b, :, cols], 1, 1)
            scores = scores * jnp.exp(jnp.where(causal, bc - bc.T, -1e30))
            scores = jnp.where(causal, scores, 0.0)
            q_in = lqD[b, :, cols]
            O[b, :, cols] = dot(scores.astype(bf16), vv[b, :, cols]) + dot(q_in.astype(bf16), PB[b, h], 1, 1)
            lqA[b, :, cols] = (q_in * jnp.exp(DP[b, h : h + 1, :])).astype(bf16)
        return 0

    with jax.named_scope("inner"):
        lax.fori_loop(0, NB, inner, 0)

    def decay_of(rows):
        part = rows[PIECE:MSG, :].astype(f32)
        return part[0:1, :] + part[1:2, :] + part[2:3, :]

    def row_to(z):
        return pltpu.make_async_remote_copy(
            zout, rz.at[Z], sZ.at[z], qZ.at[Z], device_id={"sp_0": z}, device_id_type=MESH
        )

    def row_from(z):
        return pltpu.make_async_remote_copy(
            zout, rz.at[z], sZ.at[z], qZ.at[z], device_id={"sp_0": z}, device_id_type=MESH
        )

    def send_row(z, _):
        row_to(z).start()
        return 0

    def take_row(z, before):
        row_from(z).wait_recv()
        rows = rz[z]
        return jnp.exp(decay_of(rows)) * before + rows[0:PIECE, :].astype(f32)

    def back_to(dm):
        m = lax.rem(M + dm, NM)
        return pltpu.make_async_remote_copy(
            rout.at[m], SIN.at[Y], sR, qR, device_id=member(m), device_id_type=MESH
        )

    back_order = sorted(range(1, NM), key=lambda d: -min(d // 2, NY - d // 2))

    @pl.when(C == 1)
    def _():
        with jax.named_scope("rswait"):
            pltpu.make_async_copy(rA.at[1:NM], rA.at[1:NM], qA).wait()

        state = jnp.zeros((PIECE, 128), f32)
        reach = jnp.zeros((1, 128), f32)
        reaches = []
        for m in range(NM):
            rows = rA[m]
            Pp[m] = state
            reaches.append(reach)
            step = decay_of(rows)
            state = jnp.exp(step) * state + rows[0:PIECE, :].astype(f32)
            reach = reach + step
        zout[0:PIECE, :] = state.astype(bf16)
        zout[PIECE:MSG, :] = decay_rows(reach)

        @pl.when(Z < NZ - 1)
        def _():
            pl.semaphore_wait(rdyZ, 1)

        lax.fori_loop(Z + 1, NZ, send_row, 0)
        with jax.named_scope("zwait"):
            before = lax.fori_loop(0, Z, take_row, jnp.zeros((PIECE, 128), f32))
        for m in range(NM):
            rout[m] = (jnp.exp(reaches[m]) * before + Pp[m]).astype(bf16)
        for dm in back_order:
            back_to(dm).start()
        SIN[Y] = rout[M]

    with jax.named_scope("backwait"):

        @pl.when(C == 1)
        def _():
            pltpu.make_async_copy(SIN.at[1:NP], SIN.at[1:NP], qR).wait()

        @pl.when(C == 0)
        def _():
            pltpu.make_async_copy(SIN, SIN, qR).wait()

    def h_right(who, r, half, slot):
        return pltpu.make_async_remote_copy(
            GG.at[who, r, half], GG.at[who, r, half], hsR.at[slot // 2], hrR.at[r, slot],
            device_id={"tp": right}, device_id_type=MESH,
        )

    def h_left(who, r, half, slot):
        return pltpu.make_async_remote_copy(
            GG.at[who, r, half], GG.at[who, r, half], hsL.at[slot // 2], hrL.at[r, slot],
            device_id={"tp": left}, device_id_type=MESH,
        )

    def readout(r, _):
        parts = []
        for h in range(2):
            cols = slice(h * 128, (h + 1) * 128)
            carried = SIN[h * (NP // 2) : (h + 1) * (NP // 2)].reshape(128, 128)
            o = O[r, :, cols] + dot(lqA[r, :, cols], carried, 1, 1)
            o = o * lax.rsqrt(jnp.mean(o * o, axis=1, keepdims=True) + EPS)
            parts.append(o * gs[r, :, cols])
        gated = jnp.concatenate(parts, axis=1).astype(bf16)
        GG[X, r] = gated.reshape(2, H, W2)
        h_right(X, r, 0, 0).start()
        h_left(X, r, 1, 0).start()
        h_right(X, r, 1, 1).start()
        h_left(X, r, 0, 1).start()
        return 0

    with jax.named_scope("readout"):
        lax.fori_loop(0, NB, readout, 0)
        ld_wo.wait()

    def forward(r):
        h_right(X, r, 0, 0).wait_recv()
        h_right(left, r, 0, 2).start()
        h_left(X, r, 1, 0).wait_recv()
        h_left(right, r, 1, 2).start()

    def square_to(dx, r):
        return pltpu.make_async_remote_copy(
            sqo.at[r], sqr.at[dx - 1, r], sS, qS.at[dx - 1, r],
            device_id={"tp": lax.rem(X + dx, NX)}, device_id_type=MESH,
        )

    for r in range(NB):
        with jax.named_scope("hfwd"):
            forward(r)

    def row_left(z, _):
        row_to(z).wait_send()
        return 0

    @pl.when(C == 1)
    def _():
        pltpu.make_async_copy(msgA.at[1:NP], msgA.at[1:NP], sA).wait()
        pltpu.make_async_copy(rout.at[1:NM], rout.at[1:NM], sR).wait()
        lax.fori_loop(Z + 1, NZ, row_left, 0)

    @pl.when(C == 0)
    def _():
        pltpu.make_async_copy(msgA, msgA, sA).wait()

    def near(r, _):
        with jax.named_scope("hnear"):
            h_right(X, r, 1, 1).wait_recv()
            h_left(X, r, 0, 1).wait_recv()
        acc = dot(GG[X, r].reshape(T, W2), WO[X])
        acc = acc + dot(GG[left, r].reshape(T, W2), WO[left])
        PJ[r] = acc + dot(GG[right, r].reshape(T, W2), WO[right])
        return 0

    lax.fori_loop(0, NB, near, 0)

    def far(r, _):
        with jax.named_scope("hfar"):
            h_right(left, r, 0, 2).wait_recv()
            h_left(right, r, 1, 2).wait_recv()
        acc = PJ[r] + dot(GG[opp, r].reshape(T, W2), WO[opp])
        PJ[r] = acc
        sq = acc * acc
        sq_hi = sq.astype(bf16)
        sq_lo = (sq - sq_hi.astype(f32)).astype(bf16)
        ones = jnp.ones((8, 512), f32).astype(bf16)
        sqo[r] = dot(ones, sq_hi, 1, 1) + dot(ones, sq_lo, 1, 1)
        for dx in (2, 1, 3):
            square_to(dx, r).start()
        return 0

    lax.fori_loop(0, NB, far, 0)

    for sem in (hsR, hsL):
        pltpu.make_async_copy(GG.at[X], GG.at[X], sem.at[0]).wait()
        pltpu.make_async_copy(GG.at[X, 0:2], GG.at[X, 0:2], sem.at[1]).wait()

    def finish(r, _):
        with jax.named_scope("sqwait"):
            for dx in (1, 2, 3):
                square_to(dx, r).wait_recv()
        total = sqo[r] + sqr[0, r] + sqr[1, r] + sqr[2, r]
        scale = lax.rsqrt(total[0:1, :] / D + EPS)
        scale = jnp.broadcast_to(scale, (T, T)).T
        for j in range(4):
            cols = slice(j * 128, (j + 1) * 128)
            out[0, pl.ds(pl.multiple_of(r * T, T), T), cols] = (
                PJ[r, :, cols] * scale * ogain[:, cols]
            ).astype(bf16)
        return 0

    lax.fori_loop(0, NB, finish, 0)

    with jax.named_scope("end"):
        pltpu.make_async_copy(sqr, sqr, sS).wait()


def shards(tokens, ing, wq, wf, wi, wg, slack, sud, hgain, wo, ogain):
    vm = pl.BlockSpec(memory_space=pltpu.VMEM)
    hb = pl.BlockSpec(memory_space=pltpu.HBM)
    dma = pltpu.SemaphoreType.DMA
    V = pltpu.VMEM
    return pl.pallas_call(
        body,
        name="layer",
        out_shape=jax.ShapeDtypeStruct((1, 512, 512), bf16),
        in_specs=[hb] * 11,
        out_specs=vm,
        scratch_shapes=[
            V((1, D), f32), V((1, W2), f32), V((2, 512), f32), V((1, 128), f32), V((1, 512), f32),
            V((T, D), bf16),
            V((NX, 4, Q, D), bf16),
            V((4, D, W2), bf16),
            V((NX, W2, 512), bf16),
            V((NB, T, W2), bf16),
            V((NB, T, W2), bf16),
            V((NB, T, W2), bf16),
            V((NB, T, W2), f32),
            V((NB, T, W2), f32),
            V((NB, 2, 128, 128), f32),
            V((NB, 2, 128, 128), bf16),
            V((NB, 2, 128), f32),
            V((NB, 2, 128), f32),
            V((NB, 2, T, T), f32),
            V((NX, T, W2), f32),
            V((NB, T, W2), f32),
            V((NP, MSG, 128), bf16),
            V((NM, MSG, 128), bf16),
            V((NM, PIECE, 128), f32),
            V((MSG, 128), bf16),
            V((NZ, MSG, 128), bf16),
            V((NM, PIECE, 128), bf16),
            V((NP, PIECE, 128), bf16),
            V((NX, NB, 2, H, W2), bf16),
            V((NB, T, 512), f32),
            V((NB, 8, 128), f32),
            V((3, NB, 8, 128), f32),
            dma((4,)), dma((5,)), dma((5,)),
            dma((2,)), dma((6,)), dma((2,)), dma((6,)),
            dma, dma,
            dma((NZ,)), dma((NZ,)),
            dma, dma,
            dma((2,)), dma((NB, 3)), dma((2,)), dma((NB, 3)),
            dma, dma((3, NB)),
            pltpu.SemaphoreType.REGULAR, pltpu.SemaphoreType.REGULAR,
        ],
        compiler_params=pltpu.CompilerParams(
            collective_id=0, has_side_effects=True, vmem_limit_bytes=40 * 1024 * 1024
        ),
    )(
        *(
            pltpu.with_memory_space_constraint(x, pltpu.HBM)
            for x in (
                tokens,
                ing.reshape(1, D),
                wq, wf, wi, wg,
                slack.reshape(1, W2),
                sud[0].T,
                hgain.reshape(1, 128),
                wo.reshape(NX, W2, 512),
                ogain.reshape(1, 512),
            )
        )
    )


def solution(mesh):
    torus = Mesh(mesh.devices.reshape(NZ, NY, NC, NX), ("sp_0", "sp_1", "sp_2", "tp"))
    in_specs = (
        P(None, SP_TP, None),
        P(),
        P(None, "tp"),
        P(None, "tp"),
        P(None, "tp"),
        P(None, "tp"),
        P("tp"),
        P(None, SP, "tp"),
        P(),
        P(None, "tp"),
        P("tp"),
    )
    out_specs = P(None, SP, "tp")
    return jax.shard_map(shards, mesh=torus, in_specs=in_specs, out_specs=out_specs, check_vma=False)
```

```python
import jax
import jax.numpy as jnp
from jax import lax
from jax.experimental import pallas as pl
from jax.experimental.pallas import tpu as pltpu
from jax.sharding import Mesh
from jax.sharding import PartitionSpec as P

D = 2048
KEY = 128
SP = ("sp_0", "sp_1", "sp_2")
SP_TP = ("sp_0", "sp_1", "sp_2", "tp")
MESH = pl.DeviceIdType.MESH
EPS = 1e-06

NZ, NY, NC, NX = 12, 8, 2, 4
NM = NY * NC
T = 128
H = T // 2
Q = T // 4
OUTER = (0, 3, 1, 2)
NB = 4
W2 = 256
NP = NY
PIECE = 256 // NP
MSG = PIECE + 8

bf16 = jnp.bfloat16
f32 = jnp.float32


def dot(a, b, ca=1, cb=0):
    return lax.dot_general(a, b, (((ca,), (cb,)), ((), ())), preferred_element_type=f32)


def split3(x):
    hi = x.astype(bf16).astype(f32)
    rest = x - hi
    mid = rest.astype(bf16).astype(f32)
    return hi, mid, rest - mid


def decay_rows(row):
    hi, mid, lo = split3(row)
    at = lax.broadcasted_iota(jnp.int32, (8, 128), 0)
    rows = jnp.where(at == 0, hi, jnp.where(at == 1, mid, jnp.where(at == 2, lo, 0.0)))
    return rows.astype(bf16)


def body(
    tokens, ing_in, wq, wf, wi, wg, slack_in, sud_in, hgain_in, wo, ogain_in, out,
    ing, slack, sud, hgain, ogain,
    xin, G, W, WO, lqA, lk, vv, lqD, gs, ST, PB, DT, DP, BC, AA, WK, O,
    msgA, rA, Pp, zout, rz, rout, SIN, GG, PJ, sqo, sqr,
    tksem, smsem, ldsem, gsR, grR, gsL, grL, sA, qA, sZ, qZ, sR, qR, hsR, hrR, hsL, hrL, sS, qS, rdyM, rdyZ,
):
    X = lax.axis_index("tp")
    Z = lax.axis_index("sp_0")
    Y = lax.axis_index("sp_1")
    C = lax.axis_index("sp_2")
    M = Y * NC + C
    right = lax.rem(X + 1, NX)
    left = lax.rem(X + NX - 1, NX)
    opp = lax.rem(X + 2, NX)

    def member(m):
        return {"sp_1": m // NC, "sp_2": lax.rem(m, NC)}

    host_y = jnp.where(Z == 0, 0, NY // 2)
    host_c = jnp.where(Z == 0, 0, 1)
    hosts_row = (Y == host_y) & (C == host_c)
    hosts_line = (Z == NZ - 1) & (C == 1)
    host = host_y * NC + host_c
    to_hear = 2 + jnp.where(hosts_row, NM - 1, 0) + jnp.where(hosts_line, NZ - 1, 0)
    barrier = pltpu.get_barrier_semaphore()

    def load_rows(k):
        rows = pl.ds(k * Q, Q)
        return pltpu.make_async_copy(tokens.at[0, rows], xin.at[rows], tksem.at[k])

    small = [
        pltpu.make_async_copy(a, b, smsem.at[i])
        for i, (a, b) in enumerate(
            ((ing_in, ing), (slack_in, slack), (sud_in, sud), (hgain_in, hgain), (ogain_in, ogain))
        )
    ]
    loads = [pltpu.make_async_copy(w, W.at[i], ldsem.at[i]) for i, w in enumerate((wq, wf, wi, wg))]
    ld_wo = pltpu.make_async_copy(wo, WO, ldsem.at[4])
    load_rows(0).start()
    small[0].start()
    for side in (right, left):
        pl.semaphore_signal(barrier, inc=1, device_id={"tp": side}, device_id_type=MESH)
    for k in OUTER[1:]:
        load_rows(k).start()

    @pl.when(jnp.logical_not(hosts_row))
    def _():
        pl.semaphore_signal(barrier, inc=1, device_id={"sp_1": host_y, "sp_2": host_c}, device_id_type=MESH)

    @pl.when((Z < NZ - 1) & (C == 1))
    def _():
        pl.semaphore_signal(barrier, inc=1, device_id={"sp_0": NZ - 1}, device_id_type=MESH)

    small[0].wait()

    def norm_rows(k):
        def some(i, _):
            at = pl.ds(pl.multiple_of(k * Q + i * 16, 16), 16)
            rows = xin[at, :].astype(f32)
            rows = rows * lax.rsqrt(jnp.mean(rows * rows, axis=1, keepdims=True) + EPS) * ing[...]
            G[X, k, pl.ds(pl.multiple_of(i * 16, 16), 16), :] = rows.astype(bf16)
            return 0

        lax.fori_loop(0, Q // 16, some, 0)

    def to_right(who, k, slot):
        return pltpu.make_async_remote_copy(
            G.at[who, k], G.at[who, k], gsR.at[slot // 4], grR.at[slot], device_id={"tp": right}, device_id_type=MESH
        )

    def to_left(who, k, slot):
        return pltpu.make_async_remote_copy(
            G.at[who, k], G.at[who, k], gsL.at[slot // 4], grL.at[slot], device_id={"tp": left}, device_id_type=MESH
        )

    with jax.named_scope("ld0"):
        load_rows(0).wait()
    with jax.named_scope("n0"):
        norm_rows(0)
        load_rows(3).wait()
        norm_rows(3)
    with jax.named_scope("barrier"):
        pl.semaphore_wait(barrier, to_hear)
    to_right(X, 0, 0).start()
    to_left(X, 3, 3).start()
    for c in loads:
        c.start()
    for c in small[1:]:
        c.start()
    ld_wo.start()
    load_rows(1).wait()
    norm_rows(1)
    to_right(X, 1, 1).start()
    load_rows(2).wait()
    norm_rows(2)
    to_left(X, 2, 2).start()
    to_right(X, 2, 2).start()
    to_left(X, 1, 1).start()
    to_right(X, 3, 3).start()
    to_left(X, 0, 0).start()

    def ready_row(k, _):
        pl.semaphore_signal(rdyM, inc=1, device_id=member(lax.rem(host + k, NM)), device_id_type=MESH)
        return 0

    def ready_line(z, _):
        pl.semaphore_signal(rdyZ, inc=1, device_id={"sp_0": z}, device_id_type=MESH)
        return 0

    @pl.when(hosts_row)
    def _():
        lax.fori_loop(1, NM, ready_row, 0)

    @pl.when(hosts_line)
    def _():
        lax.fori_loop(0, NZ - 1, ready_line, 0)

    for c in small[1:]:
        c.wait()

    t_at = lax.broadcasted_iota(jnp.int32, (T, T), 0)
    s_at = lax.broadcasted_iota(jnp.int32, (T, T), 1)
    causal = s_at <= t_at
    tri = causal.astype(f32).astype(bf16)
    for b in range(NB):
        for h in range(2):
            line = jnp.broadcast_to(sud[h : h + 1, b * T : (b + 1) * T], (T, T))
            total = jnp.sum(jnp.where(causal, line, 0.0), axis=1, keepdims=True)
            BC[b, h] = jnp.broadcast_to(total, (T, T))

    with jax.named_scope("wload"):
        for c in loads:
            c.wait()

    def block_state(b):
        x = G[b].reshape(T, D)
        f_raw = dot(x, W[1]).astype(bf16).astype(f32)
        i_raw = dot(x, W[2]).astype(bf16)
        vv[b] = i_raw
        w = slack[...] * jax.nn.sigmoid(-f_raw)
        a = jnp.log1p(-w)
        a_hi = a.astype(bf16)
        a_lo = (a - a_hi.astype(f32)).astype(bf16)
        A = dot(tri, a_hi) + dot(tri, a_lo)
        AA[b] = A
        WK[b] = w
        for h in range(2):
            cols = slice(h * 128, (h + 1) * 128)
            reach = A[:, cols] + BC[b, h]
            end = reach[T - 1 : T, :]
            DT[b, h : h + 1, :] = end
            wk = (w[:, cols] * jnp.exp(end - reach)).astype(bf16)
            ST[b, h] = dot(i_raw[:, cols], wk, 0, 0)

    def block_rest(b):
        x = G[b].reshape(T, D)
        q_raw = dot(x, W[0]).astype(bf16).astype(f32) * KEY ** (-0.5)
        lk[b] = (WK[b] * jnp.exp(-AA[b])).astype(bf16)
        q_in = q_raw * jnp.exp(AA[b])
        lqA[b] = q_in.astype(bf16)
        for h in range(2):
            cols = slice(h * 128, (h + 1) * 128)
            lqD[b, :, cols] = q_in[:, cols] * jnp.exp(BC[b, h])
        g_raw = dot(x, W[3]).astype(bf16).astype(f32)
        silu = g_raw * jax.nn.sigmoid(g_raw)
        for h in range(2):
            cols = slice(h * 128, (h + 1) * 128)
            gs[b, :, cols] = silu[:, cols] * hgain[...]

    def arrive(i, _):
        @pl.when(i == 1)
        def _():
            with jax.named_scope("g1"):
                to_right(X, 0, 0).wait_recv()
                to_right(left, 0, 4).start()
                to_left(X, 3, 3).wait_recv()
                to_left(right, 3, 4).start()
                to_right(X, 1, 1).wait_recv()
                to_right(left, 1, 5).start()
                to_left(X, 2, 2).wait_recv()
                to_left(right, 2, 5).start()
            with jax.named_scope("g2"):
                for k in (2, 3):
                    to_right(X, k, k).wait_recv()
                    to_left(X, 3 - k, 3 - k).wait_recv()

        @pl.when(i == 3)
        def _():
            with jax.named_scope("g3"):
                to_right(left, 0, 4).wait_recv()
                to_left(right, 3, 4).wait_recv()
                to_right(left, 1, 5).wait_recv()
                to_left(right, 2, 5).wait_recv()

        b = lax.rem(X + 3 * i + 3 * (i // 2) + 2 * (i // 3), NX)
        with jax.named_scope("state"):
            block_state(b)

        @pl.when(i < 3)
        def _():
            with jax.named_scope("rest"):
                block_rest(b)

        return 0

    lax.fori_loop(0, NB, arrive, 0)

    finals, totals = [], []
    for h in range(2):
        state = jnp.zeros((128, 128), f32)
        reach = jnp.zeros((1, 128), f32)
        for b in range(NB):
            PB[b, h] = state.astype(bf16)
            DP[b, h : h + 1, :] = reach
            step = DT[b, h : h + 1, :]
            state = jnp.exp(step) * state + ST[b, h]
            reach = reach + step
        finals.append(state)
        totals.append(reach)
    for h in range(2):
        rows = decay_rows(totals[h])
        for j in range(NP // 2):
            p = h * (NP // 2) + j
            msgA[p, 0:PIECE, :] = finals[h][j * PIECE : (j + 1) * PIECE, :].astype(bf16)
            msgA[p, PIECE:MSG, :] = rows

    far_first = sorted(range(NP), key=lambda d: -min(d, NP - d))

    def piece_to(dy):
        p = lax.rem(Y + dy, NP)
        return pltpu.make_async_remote_copy(
            msgA.at[p], rA.at[M], sA, qA, device_id={"sp_1": p, "sp_2": 1}, device_id_type=MESH
        )

    @pl.when(jnp.logical_not(hosts_row))
    def _():
        pl.semaphore_wait(rdyM, 1)

    for dy in far_first[:-1]:
        piece_to(dy).start()

    @pl.when(C == 0)
    def _():
        piece_to(0).start()

    @pl.when(C == 1)
    def _():
        rA[M] = msgA[Y]

    for sem, near_one in ((gsR, left), (gsL, right)):
        pltpu.make_async_copy(G.at[X], G.at[X], sem.at[0]).wait()
        pltpu.make_async_copy(G.at[near_one, 0:2], G.at[near_one, 0:2], sem.at[1]).wait()

    with jax.named_scope("rest3"):
        block_rest(opp)

    def inner(b, _):
        for h in range(2):
            cols = slice(h * 128, (h + 1) * 128)
            bc = BC[b, h]
            scores = dot(lqA[b, :, cols], lk[b, :, cols], 1, 1)
            scores = scores * jnp.exp(jnp.where(causal, bc - bc.T, -1e30))
            scores = jnp.where(causal, scores, 0.0)
            q_in = lqD[b, :, cols]
            O[b, :, cols] = dot(scores.astype(bf16), vv[b, :, cols]) + dot(q_in.astype(bf16), PB[b, h], 1, 1)
            lqA[b, :, cols] = (q_in * jnp.exp(DP[b, h : h + 1, :])).astype(bf16)
        return 0

    with jax.named_scope("inner"):
        lax.fori_loop(0, NB, inner, 0)

    def decay_of(rows):
        part = rows[PIECE:MSG, :].astype(f32)
        return part[0:1, :] + part[1:2, :] + part[2:3, :]

    def row_to(z):
        return pltpu.make_async_remote_copy(
            zout, rz.at[Z], sZ.at[z], qZ.at[Z], device_id={"sp_0": z}, device_id_type=MESH
        )

    def row_from(z):
        return pltpu.make_async_remote_copy(
            zout, rz.at[z], sZ.at[z], qZ.at[z], device_id={"sp_0": z}, device_id_type=MESH
        )

    def send_row(z, _):
        row_to(z).start()
        return 0

    def take_row(z, before):
        row_from(z).wait_recv()
        rows = rz[z]
        return jnp.exp(decay_of(rows)) * before + rows[0:PIECE, :].astype(f32)

    def back_to(dm):
        m = lax.rem(M + dm, NM)
        return pltpu.make_async_remote_copy(
            rout.at[m], SIN.at[Y], sR, qR, device_id=member(m), device_id_type=MESH
        )

    back_order = sorted(range(1, NM), key=lambda d: -min(d // 2, NY - d // 2))

    @pl.when(C == 1)
    def _():
        with jax.named_scope("rswait"):
            pltpu.make_async_copy(rA.at[1:NM], rA.at[1:NM], qA).wait()

        state = jnp.zeros((PIECE, 128), f32)
        reach = jnp.zeros((1, 128), f32)
        reaches = []
        for m in range(NM):
            rows = rA[m]
            Pp[m] = state
            reaches.append(reach)
            step = decay_of(rows)
            state = jnp.exp(step) * state + rows[0:PIECE, :].astype(f32)
            reach = reach + step
        zout[0:PIECE, :] = state.astype(bf16)
        zout[PIECE:MSG, :] = decay_rows(reach)

        @pl.when(Z < NZ - 1)
        def _():
            pl.semaphore_wait(rdyZ, 1)

        lax.fori_loop(Z + 1, NZ, send_row, 0)
        with jax.named_scope("zwait"):
            before = lax.fori_loop(0, Z, take_row, jnp.zeros((PIECE, 128), f32))
        for m in range(NM):
            rout[m] = (jnp.exp(reaches[m]) * before + Pp[m]).astype(bf16)
        for dm in back_order:
            back_to(dm).start()
        SIN[Y] = rout[M]

    with jax.named_scope("backwait"):

        @pl.when(C == 1)
        def _():
            pltpu.make_async_copy(SIN.at[1:NP], SIN.at[1:NP], qR).wait()

        @pl.when(C == 0)
        def _():
            pltpu.make_async_copy(SIN, SIN, qR).wait()

    def h_right(who, r, half, slot, on):
        return pltpu.make_async_remote_copy(
            GG.at[who, r, half], GG.at[who, r, half], hsR.at[on], hrR.at[r, slot],
            device_id={"tp": right}, device_id_type=MESH,
        )

    def h_left(who, r, half, slot, on):
        return pltpu.make_async_remote_copy(
            GG.at[who, r, half], GG.at[who, r, half], hsL.at[on], hrL.at[r, slot],
            device_id={"tp": left}, device_id_type=MESH,
        )

    def readout(r, _):
        parts = []
        for h in range(2):
            cols = slice(h * 128, (h + 1) * 128)
            carried = SIN[h * (NP // 2) : (h + 1) * (NP // 2)].reshape(128, 128)
            o = O[r, :, cols] + dot(lqA[r, :, cols], carried, 1, 1)
            o = o * lax.rsqrt(jnp.mean(o * o, axis=1, keepdims=True) + EPS)
            parts.append(o * gs[r, :, cols])
        gated = jnp.concatenate(parts, axis=1).astype(bf16)
        GG[X, r] = gated.reshape(2, H, W2)
        h_right(X, r, 0, 0, 0).start()
        h_left(X, r, 1, 0, 0).start()
        h_right(X, r, 1, 1, 0).start()
        h_left(X, r, 0, 1, 0).start()
        return 0

    with jax.named_scope("readout"):
        lax.fori_loop(0, NB, readout, 0)
        ld_wo.wait()

    def forward(r):
        h_right(X, r, 0, 0, 0).wait_recv()
        h_right(left, r, 0, 2, 1).start()
        h_left(X, r, 1, 0, 0).wait_recv()
        h_left(right, r, 1, 2, 1).start()

    def square_to(dx, r):
        return pltpu.make_async_remote_copy(
            sqo.at[r], sqr.at[r, dx - 1], sS, qS.at[r],
            device_id={"tp": lax.rem(X + dx, NX)}, device_id_type=MESH,
        )

    for r in range(NB):
        with jax.named_scope("hfwd"):
            forward(r)

    def row_left(z, _):
        row_to(z).wait_send()
        return 0

    @pl.when(C == 1)
    def _():
        pltpu.make_async_copy(msgA.at[1:NP], msgA.at[1:NP], sA).wait()
        pltpu.make_async_copy(rout.at[1:NM], rout.at[1:NM], sR).wait()
        lax.fori_loop(Z + 1, NZ, row_left, 0)

    @pl.when(C == 0)
    def _():
        pltpu.make_async_copy(msgA, msgA, sA).wait()

    def near(r, _):
        with jax.named_scope("hnear"):
            h_right(X, r, 1, 1, 0).wait_recv()
            h_left(X, r, 0, 1, 0).wait_recv()
        acc = dot(GG[X, r].reshape(T, W2), WO[X])
        acc = acc + dot(GG[left, r].reshape(T, W2), WO[left])
        PJ[r] = acc + dot(GG[right, r].reshape(T, W2), WO[right])
        return 0

    lax.fori_loop(0, NB, near, 0)

    def far(r, _):
        with jax.named_scope("hfar"):
            h_right(left, r, 0, 2, 1).wait_recv()
            h_left(right, r, 1, 2, 1).wait_recv()
        acc = PJ[r] + dot(GG[opp, r].reshape(T, W2), WO[opp])
        PJ[r] = acc
        sq = acc * acc
        sq = (sq[:, 0:128] + sq[:, 128:256]) + (sq[:, 256:384] + sq[:, 384:512])
        sq_hi = sq.astype(bf16)
        sq_lo = (sq - sq_hi.astype(f32)).astype(bf16)
        ones = jnp.ones((8, 128), f32).astype(bf16)
        sqo[r] = dot(ones, sq_hi, 1, 1) + dot(ones, sq_lo, 1, 1)
        for dx in (2, 1, 3):
            square_to(dx, r).start()
        return 0

    lax.fori_loop(0, NB, far, 0)

    for sem in (hsR, hsL):
        pltpu.make_async_copy(GG.at[X], GG.at[X], sem.at[0]).wait()
        pltpu.make_async_copy(GG.at[X, 0:2], GG.at[X, 0:2], sem.at[1]).wait()

    def finish(r, _):
        with jax.named_scope("sqwait"):
            pltpu.make_async_copy(sqr.at[r], sqr.at[r], qS.at[r]).wait()
        total = sqo[r] + sqr[r, 0] + sqr[r, 1] + sqr[r, 2]
        scale = lax.rsqrt(total[0:1, :] / D + EPS)
        scale = jnp.broadcast_to(scale, (T, T)).T
        for j in range(4):
            cols = slice(j * 128, (j + 1) * 128)
            out[0, pl.ds(pl.multiple_of(r * T, T), T), cols] = (
                PJ[r, :, cols] * scale * ogain[:, cols]
            ).astype(bf16)
        return 0

    lax.fori_loop(0, NB, finish, 0)

    with jax.named_scope("end"):
        pltpu.make_async_copy(sqr, sqr, sS).wait()


def shards(tokens, ing, wq, wf, wi, wg, slack, sud, hgain, wo, ogain):
    vm = pl.BlockSpec(memory_space=pltpu.VMEM)
    hb = pl.BlockSpec(memory_space=pltpu.HBM)
    dma = pltpu.SemaphoreType.DMA
    V = pltpu.VMEM
    return pl.pallas_call(
        body,
        name="layer",
        out_shape=jax.ShapeDtypeStruct((1, 512, 512), bf16),
        in_specs=[hb] * 11,
        out_specs=vm,
        scratch_shapes=[
            V((1, D), f32), V((1, W2), f32), V((2, 512), f32), V((1, 128), f32), V((1, 512), f32),
            V((T, D), bf16),
            V((NX, 4, Q, D), bf16),
            V((4, D, W2), bf16),
            V((NX, W2, 512), bf16),
            V((NB, T, W2), bf16),
            V((NB, T, W2), bf16),
            V((NB, T, W2), bf16),
            V((NB, T, W2), f32),
            V((NB, T, W2), f32),
            V((NB, 2, 128, 128), f32),
            V((NB, 2, 128, 128), bf16),
            V((NB, 2, 128), f32),
            V((NB, 2, 128), f32),
            V((NB, 2, T, T), f32),
            V((NX, T, W2), f32),
            V((NX, T, W2), f32),
            V((NB, T, W2), f32),
            V((NP, MSG, 128), bf16),
            V((NM, MSG, 128), bf16),
            V((NM, PIECE, 128), f32),
            V((MSG, 128), bf16),
            V((NZ, MSG, 128), bf16),
            V((NM, PIECE, 128), bf16),
            V((NP, PIECE, 128), bf16),
            V((NX, NB, 2, H, W2), bf16),
            V((NB, T, 512), f32),
            V((NB, 8, 128), f32),
            V((NB, 3, 8, 128), f32),
            dma((4,)), dma((5,)), dma((5,)),
            dma((2,)), dma((6,)), dma((2,)), dma((6,)),
            dma, dma,
            dma((NZ,)), dma((NZ,)),
            dma, dma,
            dma((2,)), dma((NB, 3)), dma((2,)), dma((NB, 3)),
            dma, dma((NB,)),
            pltpu.SemaphoreType.REGULAR, pltpu.SemaphoreType.REGULAR,
        ],
        compiler_params=pltpu.CompilerParams(
            collective_id=0, has_side_effects=True, vmem_limit_bytes=40 * 1024 * 1024
        ),
    )(
        *(
            pltpu.with_memory_space_constraint(x, pltpu.HBM)
            for x in (
                tokens,
                ing.reshape(1, D),
                wq, wf, wi, wg,
                slack.reshape(1, W2),
                sud[0].T,
                hgain.reshape(1, 128),
                wo.reshape(NX, W2, 512),
                ogain.reshape(1, 512),
            )
        )
    )


def solution(mesh):
    torus = Mesh(mesh.devices.reshape(NZ, NY, NC, NX), ("sp_0", "sp_1", "sp_2", "tp"))
    in_specs = (
        P(None, SP_TP, None),
        P(),
        P(None, "tp"),
        P(None, "tp"),
        P(None, "tp"),
        P(None, "tp"),
        P("tp"),
        P(None, SP, "tp"),
        P(),
        P(None, "tp"),
        P("tp"),
    )
    out_specs = P(None, SP, "tp")
    return jax.shard_map(shards, mesh=torus, in_specs=in_specs, out_specs=out_specs, check_vma=False)
```

```python
import jax
import jax.numpy as jnp
from jax import lax
from jax.experimental import pallas as pl
from jax.experimental.pallas import tpu as pltpu
from jax.sharding import Mesh
from jax.sharding import PartitionSpec as P

D = 2048
KEY = 128
SP = ("sp_0", "sp_1", "sp_2")
SP_TP = ("sp_0", "sp_1", "sp_2", "tp")
MESH = pl.DeviceIdType.MESH
EPS = 1e-06

NZ, NY, NC, NX = 12, 8, 2, 4
NM = NY * NC
T = 128
H = T // 2
Q = T // 4
OUTER = (0, 3, 1, 2)
NB = 4
W2 = 256
NP = NY
PIECE = 256 // NP
MSG = PIECE + 8

bf16 = jnp.bfloat16
f32 = jnp.float32


def dot(a, b, ca=1, cb=0):
    return lax.dot_general(a, b, (((ca,), (cb,)), ((), ())), preferred_element_type=f32)


def split3(x):
    hi = x.astype(bf16).astype(f32)
    rest = x - hi
    mid = rest.astype(bf16).astype(f32)
    return hi, mid, rest - mid


def decay_rows(row):
    hi, mid, lo = split3(row)
    at = lax.broadcasted_iota(jnp.int32, (8, 128), 0)
    rows = jnp.where(at == 0, hi, jnp.where(at == 1, mid, jnp.where(at == 2, lo, 0.0)))
    return rows.astype(bf16)


def body(
    tokens, ing_in, wq, wf, wi, wg, slack_in, sud_in, hgain_in, wo, ogain_in, out,
    ing, slack, sud, hgain, ogain,
    xin, G, W, WO, lqA, lk, vv, lqD, gs, ST, PB, DT, DP, BC, AA, WK, O,
    FS, TR, NI, msgA, rA, Pp, zout, rz, rout, SIN, GG, PJ, sqo, sqr,
    tksem, smsem, ldsem, gsR, grR, gsL, grL, sA, qA, sZ, qZ, sR, qR, sN, qN, hsR, hrR, hsL, hrL, sS, qS, rdyM, rdyZ,
):
    X = lax.axis_index("tp")
    Z = lax.axis_index("sp_0")
    Y = lax.axis_index("sp_1")
    C = lax.axis_index("sp_2")
    M = Y * NC + C
    right = lax.rem(X + 1, NX)
    left = lax.rem(X + NX - 1, NX)
    opp = lax.rem(X + 2, NX)

    def member(m):
        return {"sp_1": m // NC, "sp_2": lax.rem(m, NC)}

    barrier = pltpu.get_barrier_semaphore()
    for side in (right, left):
        pl.semaphore_signal(barrier, inc=1, device_id={"tp": side}, device_id_type=MESH)
    host_y = jnp.where(Z == 0, 0, NY // 2)
    host_c = jnp.where(Z == 0, 0, 1)
    hosts_row = (Y == host_y) & (C == host_c)
    hosts_line = (Z == NZ - 1) & (C == 1)
    host = host_y * NC + host_c
    to_hear = 2 + jnp.where(hosts_row, NM - 1, 0) + jnp.where(hosts_line, NZ - 1, 0)
    def load_rows(k):
        rows = pl.ds(k * Q, Q)
        return pltpu.make_async_copy(tokens.at[0, rows], xin.at[rows], tksem.at[k])

    small = [
        pltpu.make_async_copy(a, b, smsem.at[i])
        for i, (a, b) in enumerate(
            ((ing_in, ing), (slack_in, slack), (sud_in, sud), (hgain_in, hgain), (ogain_in, ogain))
        )
    ]
    loads = [pltpu.make_async_copy(w, W.at[i], ldsem.at[0]) for i, w in enumerate((wq, wf, wi, wg))]
    ld_wo = pltpu.make_async_copy(wo, WO, ldsem.at[1])
    load_rows(0).start()
    small[0].start()
    for k in OUTER[1:]:
        load_rows(k).start()

    @pl.when(jnp.logical_not(hosts_row))
    def _():
        pl.semaphore_signal(barrier, inc=1, device_id={"sp_1": host_y, "sp_2": host_c}, device_id_type=MESH)

    @pl.when((Z < NZ - 1) & (C == 1))
    def _():
        pl.semaphore_signal(barrier, inc=1, device_id={"sp_0": NZ - 1}, device_id_type=MESH)

    small[0].wait()

    def norm_rows(k):
        def some(i, _):
            at = pl.ds(pl.multiple_of(k * Q + i * 16, 16), 16)
            rows = xin[at, :].astype(f32)
            rows = rows * lax.rsqrt(jnp.mean(rows * rows, axis=1, keepdims=True) + EPS) * ing[...]
            G[X, k, pl.ds(pl.multiple_of(i * 16, 16), 16), :] = rows.astype(bf16)
            return 0

        lax.fori_loop(0, Q // 16, some, 0)

    def to_right(who, k, slot):
        return pltpu.make_async_remote_copy(
            G.at[who, k], G.at[who, k], gsR.at[slot // 4], grR.at[slot], device_id={"tp": right}, device_id_type=MESH
        )

    def to_left(who, k, slot):
        return pltpu.make_async_remote_copy(
            G.at[who, k], G.at[who, k], gsL.at[slot // 4], grL.at[slot], device_id={"tp": left}, device_id_type=MESH
        )

    with jax.named_scope("ld0"):
        load_rows(0).wait()
    with jax.named_scope("n0"):
        norm_rows(0)
        load_rows(3).wait()
        norm_rows(3)
    with jax.named_scope("barrier"):
        pl.semaphore_wait(barrier, to_hear)
    to_right(X, 0, 0).start()
    to_left(X, 3, 3).start()
    for c in loads:
        c.start()
    for c in small[1:]:
        c.start()
    ld_wo.start()
    load_rows(1).wait()
    norm_rows(1)
    to_right(X, 1, 1).start()
    load_rows(2).wait()
    norm_rows(2)
    to_left(X, 2, 2).start()
    to_right(X, 2, 2).start()
    to_left(X, 1, 1).start()
    to_right(X, 3, 3).start()
    to_left(X, 0, 0).start()

    def ready_row(k, _):
        pl.semaphore_signal(rdyM, inc=1, device_id=member(lax.rem(host + k, NM)), device_id_type=MESH)
        return 0

    def ready_line(z, _):
        pl.semaphore_signal(rdyZ, inc=1, device_id={"sp_0": z}, device_id_type=MESH)
        return 0

    @pl.when(hosts_row)
    def _():
        lax.fori_loop(1, NM, ready_row, 0)

    @pl.when(hosts_line)
    def _():
        lax.fori_loop(0, NZ - 1, ready_line, 0)

    for c in small[1:]:
        c.wait()

    t_at = lax.broadcasted_iota(jnp.int32, (T, T), 0)
    s_at = lax.broadcasted_iota(jnp.int32, (T, T), 1)
    causal = s_at <= t_at
    tri = causal.astype(f32).astype(bf16)
    for b in range(NB):
        for h in range(2):
            line = jnp.broadcast_to(sud[h : h + 1, b * T : (b + 1) * T], (T, T))
            total = jnp.sum(jnp.where(causal, line, 0.0), axis=1, keepdims=True)
            BC[b, h] = jnp.broadcast_to(total, (T, T))

    with jax.named_scope("wload"):
        pltpu.make_async_copy(W, W, ldsem.at[0]).wait()

    def block_state(b):
        x = G[b].reshape(T, D)
        f_raw = dot(x, W[1]).astype(bf16).astype(f32)
        i_raw = dot(x, W[2]).astype(bf16)
        vv[b] = i_raw
        w = slack[...] * jax.nn.sigmoid(-f_raw)
        a = jnp.log1p(-w)
        a_hi = a.astype(bf16)
        a_lo = (a - a_hi.astype(f32)).astype(bf16)
        A = dot(tri, a_hi) + dot(tri, a_lo)
        AA[b] = A
        WK[b] = w
        for h in range(2):
            cols = slice(h * 128, (h + 1) * 128)
            reach = A[:, cols] + BC[b, h]
            end = reach[T - 1 : T, :]
            DT[b, h : h + 1, :] = end
            wk = (w[:, cols] * jnp.exp(end - reach)).astype(bf16)
            ST[b, h] = dot(i_raw[:, cols], wk, 0, 0)

    def block_rest(b):
        x = G[b].reshape(T, D)
        q_raw = dot(x, W[0]).astype(bf16).astype(f32) * KEY ** (-0.5)
        lk[b] = (WK[b] * jnp.exp(-AA[b])).astype(bf16)
        q_in = q_raw * jnp.exp(AA[b])
        lqA[b] = q_in.astype(bf16)
        for h in range(2):
            cols = slice(h * 128, (h + 1) * 128)
            lqD[b, :, cols] = q_in[:, cols] * jnp.exp(BC[b, h])
        g_raw = dot(x, W[3]).astype(bf16).astype(f32)
        silu = g_raw * jax.nn.sigmoid(g_raw)
        for h in range(2):
            cols = slice(h * 128, (h + 1) * 128)
            gs[b, :, cols] = silu[:, cols] * hgain[...]

    def arrive(i, _):
        @pl.when(i == 1)
        def _():
            with jax.named_scope("g1"):
                to_right(X, 0, 0).wait_recv()
                to_right(left, 0, 4).start()
                to_left(X, 3, 3).wait_recv()
                to_left(right, 3, 4).start()
                to_right(X, 1, 1).wait_recv()
                to_right(left, 1, 5).start()
                to_left(X, 2, 2).wait_recv()
                to_left(right, 2, 5).start()
            with jax.named_scope("g2"):
                for k in (2, 3):
                    to_right(X, k, k).wait_recv()
                    to_left(X, 3 - k, 3 - k).wait_recv()

        @pl.when(i == 3)
        def _():
            with jax.named_scope("g3"):
                to_right(left, 0, 4).wait_recv()
                to_left(right, 3, 4).wait_recv()
                to_right(left, 1, 5).wait_recv()
                to_left(right, 2, 5).wait_recv()

        b = lax.rem(X + 3 * i + 3 * (i // 2) + 2 * (i // 3), NX)
        with jax.named_scope("state"):
            block_state(b)

        @pl.when(i < 3)
        def _():
            with jax.named_scope("rest"):
                block_rest(b)

        return 0

    lax.fori_loop(0, NB, arrive, 0)

    finals, totals = [], []
    for h in range(2):
        state = jnp.zeros((128, 128), f32)
        reach = jnp.zeros((1, 128), f32)
        for b in range(NB):
            PB[b, h] = state.astype(bf16)
            DP[b, h : h + 1, :] = reach
            step = DT[b, h : h + 1, :]
            state = jnp.exp(step) * state + ST[b, h]
            reach = reach + step
        finals.append(state)
        totals.append(reach)
        FS[h] = state
        TR[h : h + 1, :] = reach
    for h in range(2):
        rows = decay_rows(totals[h])
        for j in range(NP // 2):
            p = h * (NP // 2) + j
            msgA[p, 0:PIECE, :] = finals[h][j * PIECE : (j + 1) * PIECE, :].astype(bf16)
            msgA[p, PIECE:MSG, :] = rows

    far_first = sorted(range(NP), key=lambda d: -min(d, NP - d))

    def piece_to(dy):
        p = lax.rem(Y + dy, NP)
        return pltpu.make_async_remote_copy(
            msgA.at[p], rA.at[M], sA, qA, device_id={"sp_1": p, "sp_2": 1}, device_id_type=MESH
        )

    @pl.when(jnp.logical_not(hosts_row))
    def _():
        pl.semaphore_wait(rdyM, 1)

    for dy in far_first[:-1]:
        piece_to(dy).start()

    @pl.when(C == 0)
    def _():
        piece_to(0).start()

    @pl.when(C == 1)
    def _():
        rA[M] = msgA[Y]

    for sem, near_one in ((gsR, left), (gsL, right)):
        pltpu.make_async_copy(G.at[X], G.at[X], sem.at[0]).wait()
        pltpu.make_async_copy(G.at[near_one, 0:2], G.at[near_one, 0:2], sem.at[1]).wait()

    with jax.named_scope("rest3"):
        block_rest(opp)

    def inner(b, _):
        for h in range(2):
            cols = slice(h * 128, (h + 1) * 128)
            bc = BC[b, h]
            scores = dot(lqA[b, :, cols], lk[b, :, cols], 1, 1)
            scores = scores * jnp.exp(jnp.where(causal, bc - bc.T, -1e30))
            scores = jnp.where(causal, scores, 0.0)
            q_in = lqD[b, :, cols]
            O[b, :, cols] = dot(scores.astype(bf16), vv[b, :, cols]) + dot(q_in.astype(bf16), PB[b, h], 1, 1)
            lqA[b, :, cols] = (q_in * jnp.exp(DP[b, h : h + 1, :])).astype(bf16)
        return 0

    with jax.named_scope("inner"):
        lax.fori_loop(0, NB, inner, 0)

    def decay_of(rows):
        part = rows[PIECE:MSG, :].astype(f32)
        return part[0:1, :] + part[1:2, :] + part[2:3, :]

    def row_to(z):
        return pltpu.make_async_remote_copy(
            zout, rz.at[Z], sZ.at[z], qZ.at[Z], device_id={"sp_0": z}, device_id_type=MESH
        )

    def row_from(z):
        return pltpu.make_async_remote_copy(
            zout, rz.at[z], sZ.at[z], qZ.at[z], device_id={"sp_0": z}, device_id_type=MESH
        )

    def send_row(z, _):
        row_to(z).start()
        return 0

    def take_row(z, before):
        row_from(z).wait_recv()
        rows = rz[z]
        return jnp.exp(decay_of(rows)) * before + rows[0:PIECE, :].astype(f32)

    def back_to(dy):
        y = lax.rem(Y + dy, NY)
        return pltpu.make_async_remote_copy(
            rout.at[y], SIN.at[Y], sR, qR, device_id={"sp_1": y, "sp_2": 0}, device_id_type=MESH
        )

    def pass_on():
        return pltpu.make_async_remote_copy(NI, SIN, sN, qN, device_id={"sp_2": 1}, device_id_type=MESH)

    @pl.when(C == 1)
    def _():
        with jax.named_scope("rswait"):
            pltpu.make_async_copy(rA.at[1:NM], rA.at[1:NM], qA).wait()

        state = jnp.zeros((PIECE, 128), f32)
        reach = jnp.zeros((1, 128), f32)
        reaches = []
        for m in range(NM):
            rows = rA[m]
            Pp[m] = state
            reaches.append(reach)
            step = decay_of(rows)
            state = jnp.exp(step) * state + rows[0:PIECE, :].astype(f32)
            reach = reach + step
        zout[0:PIECE, :] = state.astype(bf16)
        zout[PIECE:MSG, :] = decay_rows(reach)

        @pl.when(Z < NZ - 1)
        def _():
            pl.semaphore_wait(rdyZ, 1)

        lax.fori_loop(Z + 1, NZ, send_row, 0)
        with jax.named_scope("zwait"):
            before = lax.fori_loop(0, Z, take_row, jnp.zeros((PIECE, 128), f32))
        for y in range(NY):
            rout[y] = (jnp.exp(reaches[NC * y]) * before + Pp[NC * y]).astype(bf16)
        for dy in far_first:
            back_to(dy).start()

    with jax.named_scope("backwait"):

        @pl.when(C == 0)
        def _():
            pltpu.make_async_copy(SIN, SIN, qR).wait()
            for h in range(2):
                keep = jnp.exp(TR[h : h + 1, :])
                for j in range(NP // 2):
                    p = h * (NP // 2) + j
                    mine = FS[h, j * PIECE : (j + 1) * PIECE, :]
                    NI[p] = (keep * SIN[p].astype(f32) + mine).astype(bf16)
            pass_on().start()

        @pl.when(C == 1)
        def _():
            pass_on().wait_recv()

    def h_right(who, r, half, slot, on):
        return pltpu.make_async_remote_copy(
            GG.at[who, r, half], GG.at[who, r, half], hsR.at[on], hrR.at[slot],
            device_id={"tp": right}, device_id_type=MESH,
        )

    def h_left(who, r, half, slot, on):
        return pltpu.make_async_remote_copy(
            GG.at[who, r, half], GG.at[who, r, half], hsL.at[on], hrL.at[slot],
            device_id={"tp": left}, device_id_type=MESH,
        )

    def readout(r, _):
        parts = []
        for h in range(2):
            cols = slice(h * 128, (h + 1) * 128)
            carried = SIN[h * (NP // 2) : (h + 1) * (NP // 2)].reshape(128, 128)
            o = O[r, :, cols] + dot(lqA[r, :, cols], carried, 1, 1)
            o = o * lax.rsqrt(jnp.mean(o * o, axis=1, keepdims=True) + EPS)
            parts.append(o * gs[r, :, cols])
        gated = jnp.concatenate(parts, axis=1).astype(bf16)
        GG[X, r] = gated.reshape(2, H, W2)
        h_right(X, r, 0, r, 0).start()
        h_left(X, r, 1, r, 0).start()
        h_right(X, r, 1, 8, 0).start()
        h_left(X, r, 0, 8, 0).start()
        return 0

    with jax.named_scope("readout"):
        lax.fori_loop(0, NB, readout, 0)
        ld_wo.wait()

    def forward(r):
        h_right(X, r, 0, r, 0).wait_recv()
        h_right(left, r, 0, NB + r, 1).start()
        h_left(X, r, 1, r, 0).wait_recv()
        h_left(right, r, 1, NB + r, 1).start()

    def square_to(dx, r):
        return pltpu.make_async_remote_copy(
            sqo.at[r], sqr.at[r, dx - 1], sS, qS.at[r],
            device_id={"tp": lax.rem(X + dx, NX)}, device_id_type=MESH,
        )

    for r in range(NB):
        with jax.named_scope("hfwd"):
            forward(r)

    def row_left(z, _):
        row_to(z).wait_send()
        return 0

    @pl.when(C == 1)
    def _():
        pltpu.make_async_copy(msgA.at[1:NP], msgA.at[1:NP], sA).wait()
        pltpu.make_async_copy(rout, rout, sR).wait()
        lax.fori_loop(Z + 1, NZ, row_left, 0)

    @pl.when(C == 0)
    def _():
        pltpu.make_async_copy(msgA, msgA, sA).wait()
        pass_on().wait_send()

    with jax.named_scope("hnear"):
        for sem in (hrR, hrL):
            pltpu.make_async_copy(GG.at[X, 0:2], GG.at[X, 0:2], sem.at[2 * NB]).wait()

    def near(r, _):
        acc = dot(GG[X, r].reshape(T, W2), WO[X])
        acc = acc + dot(GG[left, r].reshape(T, W2), WO[left])
        PJ[r] = acc + dot(GG[right, r].reshape(T, W2), WO[right])
        return 0

    lax.fori_loop(0, NB, near, 0)

    def far(r, _):
        with jax.named_scope("hfar"):
            h_right(left, r, 0, NB + r, 1).wait_recv()
            h_left(right, r, 1, NB + r, 1).wait_recv()
        acc = PJ[r] + dot(GG[opp, r].reshape(T, W2), WO[opp])
        PJ[r] = acc
        sq = acc * acc
        sq = (sq[:, 0:128] + sq[:, 128:256]) + (sq[:, 256:384] + sq[:, 384:512])
        sq_hi = sq.astype(bf16)
        sq_lo = (sq - sq_hi.astype(f32)).astype(bf16)
        ones = jnp.ones((8, 128), f32).astype(bf16)
        sqo[r] = dot(ones, sq_hi, 1, 1) + dot(ones, sq_lo, 1, 1)
        for dx in (2, 1, 3):
            square_to(dx, r).start()
        return 0

    lax.fori_loop(0, NB, far, 0)

    for sem in (hsR, hsL):
        pltpu.make_async_copy(GG.at[X], GG.at[X], sem.at[0]).wait()
        pltpu.make_async_copy(GG.at[X, 0:2], GG.at[X, 0:2], sem.at[1]).wait()

    def finish(r, _):
        with jax.named_scope("sqwait"):
            pltpu.make_async_copy(sqr.at[r], sqr.at[r], qS.at[r]).wait()
        total = sqo[r] + sqr[r, 0] + sqr[r, 1] + sqr[r, 2]
        scale = lax.rsqrt(total[0:1, :] / D + EPS)
        scale = jnp.broadcast_to(scale, (T, T)).T
        for j in range(4):
            cols = slice(j * 128, (j + 1) * 128)
            out[0, pl.ds(pl.multiple_of(r * T, T), T), cols] = (
                PJ[r, :, cols] * scale * ogain[:, cols]
            ).astype(bf16)
        return 0

    lax.fori_loop(0, NB, finish, 0)

    with jax.named_scope("end"):
        pltpu.make_async_copy(sqr, sqr, sS).wait()


def shards(tokens, ing, wq, wf, wi, wg, slack, sud, hgain, wo, ogain):
    vm = pl.BlockSpec(memory_space=pltpu.VMEM)
    hb = pl.BlockSpec(memory_space=pltpu.HBM)
    dma = pltpu.SemaphoreType.DMA
    V = pltpu.VMEM
    return pl.pallas_call(
        body,
        name="layer",
        out_shape=jax.ShapeDtypeStruct((1, 512, 512), bf16),
        in_specs=[hb] * 11,
        out_specs=vm,
        scratch_shapes=[
            V((1, D), f32), V((1, W2), f32), V((2, 512), f32), V((1, 128), f32), V((1, 512), f32),
            V((T, D), bf16),
            V((NX, 4, Q, D), bf16),
            V((4, D, W2), bf16),
            V((NX, W2, 512), bf16),
            V((NB, T, W2), bf16),
            V((NB, T, W2), bf16),
            V((NB, T, W2), bf16),
            V((NB, T, W2), f32),
            V((NB, T, W2), f32),
            V((NB, 2, 128, 128), f32),
            V((NB, 2, 128, 128), bf16),
            V((NB, 2, 128), f32),
            V((NB, 2, 128), f32),
            V((NB, 2, T, T), f32),
            V((NX, T, W2), f32),
            V((NX, T, W2), f32),
            V((NB, T, W2), f32),
            V((2, 128, 128), f32),
            V((2, 128), f32),
            V((NP, PIECE, 128), bf16),
            V((NP, MSG, 128), bf16),
            V((NM, MSG, 128), bf16),
            V((NM, PIECE, 128), f32),
            V((MSG, 128), bf16),
            V((NZ, MSG, 128), bf16),
            V((NP, PIECE, 128), bf16),
            V((NP, PIECE, 128), bf16),
            V((NX, NB, 2, H, W2), bf16),
            V((NB, T, 512), f32),
            V((NB, 8, 128), f32),
            V((NB, 3, 8, 128), f32),
            dma((4,)), dma((5,)), dma((2,)),
            dma((2,)), dma((6,)), dma((2,)), dma((6,)),
            dma, dma,
            dma((NZ,)), dma((NZ,)),
            dma, dma, dma, dma,
            dma((2,)), dma((2 * NB + 1,)), dma((2,)), dma((2 * NB + 1,)),
            dma, dma((NB,)),
            pltpu.SemaphoreType.REGULAR, pltpu.SemaphoreType.REGULAR,
        ],
        compiler_params=pltpu.CompilerParams(
            collective_id=0, has_side_effects=True, vmem_limit_bytes=40 * 1024 * 1024
        ),
    )(
        *(
            pltpu.with_memory_space_constraint(x, pltpu.HBM)
            for x in (
                tokens,
                ing.reshape(1, D),
                wq, wf, wi, wg,
                slack.reshape(1, W2),
                sud[0].T,
                hgain.reshape(1, 128),
                wo.reshape(NX, W2, 512),
                ogain.reshape(1, 512),
            )
        )
    )


def solution(mesh):
    torus = Mesh(mesh.devices.reshape(NZ, NY, NC, NX), ("sp_0", "sp_1", "sp_2", "tp"))
    in_specs = (
        P(None, SP_TP, None),
        P(),
        P(None, "tp"),
        P(None, "tp"),
        P(None, "tp"),
        P(None, "tp"),
        P("tp"),
        P(None, SP, "tp"),
        P(),
        P(None, "tp"),
        P("tp"),
    )
    out_specs = P(None, SP, "tp")
    return jax.shard_map(shards, mesh=torus, in_specs=in_specs, out_specs=out_specs, check_vma=False)
```
